32 devices in a mesh: ep: 8 (over z, y), tp: 4 (over x, core).
Axes of the slice: x: 2, y: 2, z: 4, core: 2. Of those that a mesh axis runs over, the one named last changes fastest.
Arguments:
- tokens: bfloat16 [1024, 2048], P('ep'), may hold values from -6 to 6
- norm_gain: bfloat16 [2048], replicated, may hold values from 0.099609375 to 1.8984375
- expert_ids: int32 [1024, 2], P('ep'), may hold values from 0 to 7, all different within a row; in each aligned block of 128 rows (0 to 127, 128 to 255, ...) at most 48 rows name the same one
- route_weights: float32 [1024, 2], P('ep'), may hold values from 0.2 to 1.5
- gate_weight: bfloat16 [8, 2048, 512], P('ep', None, 'tp'), may hold values from -0.125 to 0.125
- up_weight: bfloat16 [8, 2048, 512], P('ep', None, 'tp'), may hold values from -0.125 to 0.125
- down_weight: bfloat16 [8, 512, 2048], P('ep', 'tp'), may hold values from -0.25 to 0.25
- shared_gate: bfloat16 [2048, 512], P(None, 'tp'), may hold values from -0.125 to 0.125
- shared_up: bfloat16 [2048, 512], P(None, 'tp'), may hold values from -0.125 to 0.125
- shared_down: bfloat16 [512, 2048], P('tp'), may hold values from -0.25 to 0.25
Outputs:
- mixed: bfloat16 [1024, 2048], P('ep', 'tp')
The draws below stay inside these ranges and needn't reach their ends.
Inputs may be any that keep to these rules, and one draw needn't show every extreme that they name: `expert_ids`: each row names 2 different experts. Among the rows of one index of ep (aligned blocks of 128 rows) no expert is named more than 48 times, a bound that some block reaches.
All inputs are finite; a program needn't handle non-finite values.
Results may differ from the reference program's by a relative error of at most 0.012.
Values may be sent and summed in bfloat16 or wider, within the bound.
A program may use at most 64 MiB of HBM per device.

```python
import math
import jax
import jax.numpy as jnp
import numpy as np
from jax import lax

D = 2048
FF = 512
TOP_K = 2
TOK_GRP = 128
EXPERTS = 8
TOKENS = 1024
CAPACITY = 48
N_EP = 8
N_TP = 4


def shard_levels(own_key, extent, cuts, low, high):
    gain = 1.0
    for axis_at, parts in cuts:
        draws = jax.random.uniform(jax.random.fold_in(jax.random.fold_in(own_key, 6), axis_at), (parts,), jnp.float32, low / len(cuts), high / len(cuts))
        gain = gain * jnp.repeat(jnp.exp(draws), extent[axis_at] // parts).reshape((-1,) + (1,) * (len(extent) - 1 - axis_at))
    return gain


def assign_block(rng, own, number, rows, count, top, bound, lean):
    sequence = jax.random.permutation(rng, count)
    crowded, common = portions_of(count, rows * top, bound, lean, True), portions_of(count, rows * top, bound, lean, False)
    places = jnp.arange(count)

    def named(tallies, offset_by):
        used = int((tallies > 0).sum())
        fixed = max(1, used // 4)
        moved = fixed + (places - fixed + offset_by * (used - fixed)) % max(1, count - fixed)
        return jnp.zeros((count,), jnp.int32).at[sequence[jnp.where(places < fixed, places, moved)]].set(jnp.asarray(tallies, jnp.int32))

    tallies = jnp.where(number % 4 == 0, named(crowded, number // 4), named(common, number - number // 4 - 1))
    mixed = jax.random.permutation(jax.random.fold_in(own, 3), count)
    source_of, sink = mixed[0:count // 2 * 2:2], mixed[1:count // 2 * 2:2]
    room = jnp.minimum(tallies[source_of] - 1, bound - tallies[sink]) // 2
    room = jnp.where((source_of == sequence[0]) | (sink == sequence[0]) | (tallies[sink] == 0), 0, jnp.maximum(room, 0))
    moved = jax.random.randint(jax.random.fold_in(own, 4), (count // 2,), 0, 1 << 20) % (room + 1)
    tallies = tallies.at[source_of].add(-moved).at[sink].add(moved)
    labels = jnp.searchsorted(jnp.cumsum(tallies), jnp.arange(rows * top), side="right").astype(jnp.int32)
    grid = labels.reshape(top, rows).T
    grid = grid[jax.random.permutation(jax.random.fold_in(own, 1), rows)]
    offset_by = jax.random.randint(jax.random.fold_in(own, 2), (rows, 1), 0, top)
    return jnp.take_along_axis(grid, (jnp.arange(top)[None, :] + offset_by) % top, axis=1)


def portions_of(amount, total, reach, slope, full):
    loads = [(1 << 20) // math.isqrt(standing ** slope) + 1 for standing in range(1, amount + 1)]
    largest = reach if full else min(reach, max(-(-total // amount), total * loads[0] // sum(loads)))
    least = 1 if total - largest >= amount - 1 else 0
    given, spare = [largest] + [least] * (amount - 1), total - largest - least * (amount - 1)
    while spare > 0:
        candidates = [i for i in range(1, amount) if given[i] < largest] or [i for i in range(1, amount) if given[i] < reach]
        whole, remaining = sum([loads[i] for i in candidates]), spare
        for i in candidates:
            more = min(reach - given[i], max(1, remaining * loads[i] // whole), spare)
            given[i] = given[i] + more
            spare = spare - more
    return np.array(given)


def centred(key, shape, spread, reach, shards=(), kind=jnp.bfloat16):
    drawn = jax.random.normal(key, shape, jnp.float32) * spread
    if len(shards) > 0:
        drawn = shard_levels(key, shape, shards, -0.22, 0.18) * drawn
    return jnp.clip(drawn, min=-reach, max=reach).astype(kind)


def setup_inputs(seed: int = 0) -> dict:
    splits = jax.random.split(jax.random.key(seed), 11)
    tokens = centred(splits[0], (TOKENS, D), 1.0, 6.0, ((0, 8),))
    norm_gain = jnp.clip(1.0 + 0.18 * jax.random.normal(splits[1], (D,), jnp.float32), 0.099609375, 1.8984375).astype(jnp.bfloat16)
    expert_ids_keys = jax.random.split(jax.random.fold_in(splits[2], 1), TOKENS // TOK_GRP)
    expert_ids_turns = jax.random.permutation(jax.random.fold_in(splits[2], 3), TOKENS // TOK_GRP)
    expert_ids = jax.vmap(lambda own, number: assign_block(jax.random.fold_in(splits[2], 2), own, number, TOK_GRP, EXPERTS, TOP_K, CAPACITY, 2))(expert_ids_keys, expert_ids_turns).reshape((TOKENS, TOP_K))
    route_weights = jnp.clip(0.2 + 1.3 * jax.random.uniform(splits[3], (TOKENS, TOP_K), jnp.float32) ** shard_levels(splits[3], (TOKENS, TOP_K), ((0, 8),), -0.2, 0.2), 0.2, 1.5)
    gate_weight = centred(splits[4], (EXPERTS, D, FF), D ** -0.5, 0.125, ((0, 8), (2, 4)))
    up_weight = centred(splits[5], (EXPERTS, D, FF), D ** -0.5, 0.125, ((0, 8), (2, 4)))
    down_weight = centred(splits[6], (EXPERTS, FF, D), FF ** -0.5, 0.25, ((0, 8), (1, 4)))
    shared_gate = centred(splits[7], (D, FF), D ** -0.5, 0.125, ((1, 4),))
    shared_up = centred(splits[8], (D, FF), D ** -0.5, 0.125, ((1, 4),))
    shared_down = centred(splits[9], (FF, D), FF ** -0.5, 0.25, ((0, 4),))
    return dict(tokens=tokens, norm_gain=norm_gain, expert_ids=expert_ids, route_weights=route_weights, gate_weight=gate_weight, up_weight=up_weight, down_weight=down_weight, shared_gate=shared_gate, shared_up=shared_up, shared_down=shared_down)


norm_eps = 1e-06

def project(rows, w_gate, w_up, w_down):
    gate = jnp.dot(rows, w_gate, preferred_element_type=jnp.float32)
    upper = jnp.dot(rows, w_up, preferred_element_type=jnp.float32)
    hidden = (jax.nn.silu(gate) * upper).astype(jnp.bfloat16)
    block = FF // N_TP
    total = jnp.zeros((rows.shape[0], w_down.shape[1]), jnp.float32)
    for index in range(N_TP):
        piece = jnp.dot(hidden[:, index * block:(index + 1) * block], w_down[index * block:(index + 1) * block], preferred_element_type=jnp.float32).astype(jnp.bfloat16)
        piece = lax.optimization_barrier(piece)
        total = total + piece.astype(jnp.float32)
    return total

def reference(tokens, norm_gain, expert_ids, route_weights, gate_weight, up_weight, down_weight, shared_gate, shared_up, shared_down):
    values = tokens.astype(jnp.float32)
    normed = (values * lax.rsqrt(lax.optimization_barrier(jnp.mean(values * values, axis=-1, keepdims=True)) + norm_eps) * norm_gain.astype(jnp.float32)).astype(jnp.bfloat16)
    shared = project(normed, shared_gate, shared_up, shared_down)
    flat = expert_ids.reshape(-1).astype(jnp.int32)
    pairs = flat.shape[0]
    order = jnp.argsort(flat, stable=True).astype(jnp.int32)
    counts = jnp.bincount(flat, length=EXPERTS).astype(jnp.int32)
    starts = jnp.cumsum(counts) - counts
    sorted_ids = flat[order]
    ranks = jnp.arange(pairs, dtype=jnp.int32) - starts[sorted_ids]
    slots = N_EP * CAPACITY
    table = jnp.full((EXPERTS, slots), pairs, jnp.int32).at[sorted_ids, ranks].set(order)
    padded = jnp.concatenate([normed, jnp.zeros((1, D), jnp.bfloat16)], axis=0)

    def one_expert(expert):
        index = table[expert]
        rows = padded[jnp.minimum(index // TOP_K, TOKENS)]
        return project(rows, gate_weight[expert], up_weight[expert], down_weight[expert]).astype(jnp.bfloat16)
    outputs = lax.map(one_expert, jnp.arange(EXPERTS, dtype=jnp.int32))
    per_pair = jnp.zeros((pairs + 1, D), jnp.bfloat16).at[table.reshape(-1)].set(outputs.reshape(-1, D))
    picked = per_pair[:pairs].reshape(TOKENS, TOP_K, D).astype(jnp.float32)
    total = shared + lax.optimization_barrier(jnp.sum(picked * route_weights[:, :, None], axis=1))
    return total.astype(jnp.bfloat16)
```

```python
import functools

import jax
import jax.numpy as jnp
from jax import lax
from jax.experimental import pallas as pl
from jax.experimental.pallas import tpu as pltpu
from jax.sharding import PartitionSpec as P

norm_eps = 1e-06
MESH = pl.DeviceIdType.MESH
ARRIVE, SPACING, SHARED = 2.7, 1.3, 2.0
LATENCY = (0.0, 4.0, 1.5, 2.5, 4.0)
F32, BF16 = jnp.float32, jnp.bfloat16


def round_up(value, unit):
    return (value + unit - 1) // unit * unit


def wide_kernel(
    n,
    n_tp,
    experts,
    cap,
    tokens_ref,
    gain_ref,
    ids_ref,
    rw_ref,
    wg_ref,
    wu_ref,
    wd_ref,
    sg_ref,
    su_ref,
    sd_ref,
    out_ref,
    tokens,
    gain,
    ids_v,
    rw_v,
    out_v,
    w_in,
    w_out,
    sw_in,
    sw_out,
    normed,
    rank_t,
    picks,
    send,
    rows,
    terms,
    core_in,
    x_out,
    x_in,
    back_out,
    back_in,
    sh_terms,
    sh_core_in,
    sh_x_out,
    sh_x_in,
    in_sem,
    w_sem,
    a2a_s,
    a2a_r,
    core_s,
    core_r,
    x_s,
    x_r,
    fwd_s,
    fwd_r,
    rsc_s,
    rsc_r,
    rsx_s,
    rsx_r,
    ret_s,
    ret_r,
    sh_s,
    sh_r,
):
    tok, width = tokens_ref.shape
    share = width // n_tp
    local_experts, _, ff = wg_ref.shape
    chosen = ids_ref.shape[0]
    halves = n_tp // 2
    me = lax.axis_index("ep")
    tp = lax.axis_index("tp")
    hi, lo = tp // 2, tp % 2
    partner = hi * 2 + 1 - lo

    def across(d):
        return (hi + d) % halves

    def steps(body):
        if n <= 8:
            for j in range(n):
                body(j)
        else:

            def one(j, carry):
                body(j)
                return carry

            lax.fori_loop(0, n, one, 0)

    def mirror(j):
        total, bit = 0, 1
        while bit < n:
            total = total + ((me // bit + j // bit) % 2) * bit
            bit *= 2
        return total

    even = n & (n - 1) == 0

    def source(j):
        return mirror(j) if even else (me - j + n) % n

    def target(j):
        return mirror(j) if even else (me + j) % n

    def when(cond, body):
        if isinstance(cond, bool):
            if cond:
                body()
        else:
            pl.when(cond)(body)

    firsts = [
        pltpu.make_async_copy(tokens_ref, tokens, in_sem.at[0]),
        pltpu.make_async_copy(gain_ref, gain, in_sem.at[1]),
        pltpu.make_async_copy(ids_ref, ids_v, in_sem.at[2]),
        pltpu.make_async_copy(rw_ref, rw_v, in_sem.at[3]),
    ]
    for load in firsts:
        load.start()

    barrier = pltpu.get_barrier_semaphore()

    def greet(j):
        def go():
            pl.semaphore_signal(barrier, inc=1, device_id=(target(j), tp), device_id_type=MESH)

        when(j > 0, go)

    steps(greet)
    pl.semaphore_signal(barrier, inc=1, device_id=(me, partner), device_id_type=MESH)
    for d in range(1, halves):
        pl.semaphore_signal(
            barrier, inc=1, device_id=(me, across(d) * 2 + lo), device_id_type=MESH
        )

    loads = [
        pltpu.make_async_copy(sg_ref, sw_in.at[:, pl.ds(0, ff)], w_sem.at[0]),
        pltpu.make_async_copy(su_ref, sw_in.at[:, pl.ds(ff, ff)], w_sem.at[1]),
        pltpu.make_async_copy(sd_ref, sw_out, w_sem.at[2]),
        pltpu.make_async_copy(wg_ref, w_in.at[:, :, pl.ds(0, ff)], w_sem.at[3]),
        pltpu.make_async_copy(wu_ref, w_in.at[:, :, pl.ds(ff, ff)], w_sem.at[4]),
        pltpu.make_async_copy(wd_ref, w_out, w_sem.at[5]),
    ]
    for load in loads:
        load.start()

    firsts[2].wait()
    firsts[3].wait()
    lanes = rank_t.shape[0]
    ids = [ids_v[k : k + 1, :] for k in range(chosen)]
    weights = [rw_v[k : k + 1, :] for k in range(chosen)]
    expert = lax.broadcasted_iota(jnp.int32, (lanes, tok), 0)
    named = ids[0] == expert
    for k in range(1, chosen):
        named = named | (ids[k] == expert)
    earlier = lax.broadcasted_iota(jnp.int32, (tok, tok), 0) < lax.broadcasted_iota(
        jnp.int32, (tok, tok), 1
    )
    rank = jnp.dot(
        jnp.where(named, 1.0, 0.0).astype(BF16),
        jnp.where(earlier, 1.0, 0.0).astype(BF16),
        preferred_element_type=F32,
    )
    rank_t[...] = jnp.where(named, rank, -1.0)

    firsts[0].wait()
    firsts[1].wait()
    values = tokens[...].astype(F32)
    scale = lax.rsqrt(jnp.mean(values * values, axis=-1, keepdims=True) + norm_eps)
    normed[...] = (values * scale * gain[...].astype(F32).reshape(1, width)).astype(BF16)

    chunk = local_experts * cap
    slot_row = lax.broadcasted_iota(jnp.int32, (cap, tok), 0).astype(F32)
    column = pl.ds(pl.multiple_of(tp * share, 128), share)

    def dispatch(j, features):
        p = target(j)
        parts = []
        for le in range(local_experts):
            line = rank_t[pl.ds(p * local_experts + le, 1), :]
            pick = jnp.where(slot_row == line, 1.0, 0.0).astype(BF16)
            parts.append(
                jnp.dot(pick, normed[:, features], preferred_element_type=F32).astype(BF16)
            )
        return parts

    def a2a(j):
        return pltpu.make_async_remote_copy(
            src_ref=send.at[j],
            dst_ref=rows.at[me, tp],
            send_sem=a2a_s.at[j],
            recv_sem=a2a_r.at[me],
            device_id=(target(j), tp),
            device_id_type=MESH,
        )

    def a2a_in(j):
        s = source(j)
        return pltpu.make_async_remote_copy(
            src_ref=send.at[j],
            dst_ref=rows.at[s, tp],
            send_sem=a2a_s.at[j],
            recv_sem=a2a_r.at[s],
            device_id=(target(j), tp),
            device_id_type=MESH,
        )

    pl.semaphore_wait(barrier, (n - 1) + 1 + (halves - 1))

    def dispatch_and_send(j):
        def go():
            for le, part in enumerate(dispatch(j, column)):
                send[j, pl.ds(le * cap, cap), :] = part
            a2a(j).start()

        when(j > 0, go)

    steps(dispatch_and_send)

    def core_copy(j):
        s = source(j)
        return pltpu.make_async_remote_copy(
            src_ref=rows.at[s, tp],
            dst_ref=rows.at[s, tp],
            send_sem=core_s.at[j],
            recv_sem=core_r.at[j],
            device_id=(me, partner),
            device_id_type=MESH,
        )

    def x_copy(j, d):
        s = source(j)
        return pltpu.make_async_remote_copy(
            src_ref=rows.at[s, tp],
            dst_ref=rows.at[s, tp],
            send_sem=x_s.at[j, d - 1],
            recv_sem=x_r.at[j, d - 1],
            device_id=(me, across(d) * 2 + lo),
            device_id_type=MESH,
        )

    def fwd_copy(j, d):
        s = source(j)
        held = across(halves - d) * 2 + lo
        return pltpu.make_async_remote_copy(
            src_ref=rows.at[s, held],
            dst_ref=rows.at[s, held],
            send_sem=fwd_s.at[j, d - 1],
            recv_sem=fwd_r.at[j, d - 1],
            device_id=(me, partner),
            device_id_type=MESH,
        )

    def stage_a(j):
        a2a_in(j).wait_recv()
        for d in range(1, halves):
            x_copy(j, d).start()
        core_copy(j).start()

    def stage_b(j):
        for d in range(1, halves):
            x_copy(j, d).wait_recv()
            fwd_copy(j, d).start()

    def rsc_copy(j):
        return pltpu.make_async_remote_copy(
            src_ref=terms.at[j, 1 - lo],
            dst_ref=core_in.at[j],
            send_sem=rsc_s.at[j],
            recv_sem=rsc_r.at[j],
            device_id=(me, partner),
            device_id_type=MESH,
        )

    def rsx_copy(j, d):
        return pltpu.make_async_remote_copy(
            src_ref=x_out.at[j, d - 1],
            dst_ref=x_in.at[j, d - 1],
            send_sem=rsx_s.at[j, d - 1],
            recv_sem=rsx_r.at[j, d - 1],
            device_id=(me, across(d) * 2 + lo),
            device_id_type=MESH,
        )

    def ret_copy(j):
        return pltpu.make_async_remote_copy(
            src_ref=back_out.at[j],
            dst_ref=back_in.at[me],
            send_sem=ret_s.at[j],
            recv_sem=ret_r.at[me],
            device_id=(source(j), tp),
            device_id_type=MESH,
        )

    def ret_in(j):
        g = target(j)
        return pltpu.make_async_remote_copy(
            src_ref=back_out.at[j],
            dst_ref=back_in.at[g],
            send_sem=ret_s.at[j],
            recv_sem=ret_r.at[g],
            device_id=(source(j), tp),
            device_id_type=MESH,
        )

    def hidden_of(mixed):
        gate, up = mixed[:, :ff], mixed[:, ff:]
        return (gate / (1.0 + jnp.exp(-gate)) * up).astype(BF16)

    def expert_hidden(s, le):
        total = jnp.zeros((cap, 2 * ff), F32)
        for t in range(n_tp):
            total = total + jnp.dot(
                rows[s, t, pl.ds(le * cap, cap), :],
                w_in[le, pl.ds(t * share, share), :],
                preferred_element_type=F32,
            )
        return hidden_of(total)

    def stage_c(j):
        core_copy(j).wait_recv()
        for d in range(1, halves):
            fwd_copy(j, d).wait_recv()
        for le in range(local_experts):
            hidden = expert_hidden(source(j), le)
            for t in range(n_tp):
                terms[j, t % 2, t // 2, pl.ds(le * cap, cap), :] = jnp.dot(
                    hidden,
                    w_out[le, :, pl.ds(t * share, share)],
                    preferred_element_type=F32,
                ).astype(BF16)
        rsc_copy(j).start()

    def stage_d(j):
        rsc_copy(j).wait_recv()
        for d in range(1, halves):
            h = across(d)
            x_out[j, d - 1] = (
                terms[j, lo, h].astype(F32) + core_in[j, h].astype(F32)
            ).astype(BF16)
            rsx_copy(j, d).start()

    def stage_e(j):
        total = terms[j, lo, hi].astype(F32) + core_in[j, hi].astype(F32)
        for d in range(1, halves):
            rsx_copy(j, d).wait_recv()
            total = total + x_in[j, d - 1].astype(F32)
        back_out[j] = total.astype(BF16)

        ret_copy(j).start()

    def sh_core_copy():
        return pltpu.make_async_remote_copy(
            src_ref=sh_terms.at[1 - lo],
            dst_ref=sh_core_in,
            send_sem=sh_s.at[0],
            recv_sem=sh_r.at[0],
            device_id=(me, partner),
            device_id_type=MESH,
        )

    def sh_x_copy(d):
        return pltpu.make_async_remote_copy(
            src_ref=sh_x_out.at[d - 1],
            dst_ref=sh_x_in.at[d - 1],
            send_sem=sh_s.at[d],
            recv_sem=sh_r.at[d],
            device_id=(me, across(d) * 2 + lo),
            device_id_type=MESH,
        )

    def make_picks():
        slots = n * chunk
        place = rank + (expert * cap).astype(F32)
        lines = [
            jnp.sum(jnp.where(ids[k] == expert, place, 0.0), axis=0, keepdims=True)
            for k in range(chosen)
        ] + weights
        for le in range(local_experts):
            mine = me * local_experts + le
            lines.append(rank_t[pl.ds(mine, 1), :])
            weight = jnp.zeros((1, tok), F32)
            for k in range(chosen):
                weight = weight + jnp.where(ids[k] == mine, weights[k], 0.0)
            lines.append(weight)
        at_row = lax.broadcasted_iota(jnp.int32, (tok, tok), 0)
        table = jnp.zeros((tok, tok), F32)
        for index, line in enumerate(lines):
            table = jnp.where(at_row == index, line, table)
        table = table.T
        spot = lax.broadcasted_iota(jnp.int32, (tok, slots), 1).astype(F32)
        for k in range(chosen):
            picks[k] = jnp.where(spot == table[:, k : k + 1], 1.0, 0.0).astype(BF16)
        return table

    def shared_first():
        for load in loads[:3]:
            load.wait()
        hidden = hidden_of(jnp.dot(normed[...], sw_in[...], preferred_element_type=F32))
        slot = lax.broadcasted_iota(jnp.int32, (tok, cap), 1).astype(F32)
        table = make_picks()
        for load in loads[3:]:
            load.wait()
        own = []
        for le in range(local_experts):
            for t in range(n_tp):
                features = pl.ds(t * share, share)
                rows[me, t, pl.ds(le * cap, cap), :] = dispatch(0, features)[le]
            own.append(expert_hidden(me, le))
        for t in range(n_tp):
            features = pl.ds(t * share, share)
            total = jnp.dot(hidden, sw_out[:, features], preferred_element_type=F32)
            for le in range(local_experts):
                at = 2 * chosen + 2 * le
                pick = jnp.where(slot == table[:, at : at + 1], 1.0, 0.0).astype(BF16)
                term = jnp.dot(
                    own[le], w_out[le, :, features], preferred_element_type=F32
                ).astype(BF16)
                total = total + table[:, at + 1 : at + 2] * jnp.dot(
                    pick, term, preferred_element_type=F32
                )
            sh_terms[t % 2, t // 2] = total.astype(BF16)
        sh_core_copy().start()
        return [table[:, chosen + k : chosen + k + 1] for k in range(chosen)]

    def shared_second():
        sh_core_copy().wait_recv()
        for d in range(1, halves):
            h = across(d)
            sh_x_out[d - 1] = (sh_terms[lo, h].astype(F32) + sh_core_in[h].astype(F32)).astype(
                BF16
            )
            sh_x_copy(d).start()

    back_in[me] = jnp.zeros((chunk, share), BF16)
    route = shared_first()

    stages = (stage_a, stage_b, stage_c, stage_d, stage_e)

    if n <= 8:
        order = []
        for j in range(1, n):
            at = ARRIVE + SPACING * (j - 1)
            for index, stage in enumerate(stages):
                at += LATENCY[index]
                order.append((at, index, j))
        order.append((SHARED, -1, 0))
        for _, index, j in sorted(order):
            if index < 0:
                shared_second()
            else:
                stages[index](j)
    else:
        shared_second()
        lags = (0, 2, 3, 4, 6)

        def one(i, carry):
            for lag, stage in zip(lags, stages):
                pl.when((i - lag >= 1) & (i - lag < n))(functools.partial(stage, i - lag))
            return carry

        lax.fori_loop(1, n + lags[-1], one, 0)

    total = sh_terms[lo, hi].astype(F32) + sh_core_in[hi].astype(F32)
    for d in range(1, halves):
        sh_x_copy(d).wait_recv()
        total = total + sh_x_in[d - 1].astype(F32)

    steps(lambda j: when(j > 0, lambda: ret_in(j).wait_recv()))
    came = back_in[...].reshape(n * chunk, share)
    for k in range(chosen):
        total = total + route[k] * jnp.dot(
            picks[k], came, preferred_element_type=F32
        )
    out_v[...] = total.astype(BF16)
    result = pltpu.make_async_copy(out_v, out_ref, in_sem.at[0])
    result.start()

    def drain(j):
        def far():
            a2a(j).wait_send()
            ret_copy(j).wait_send()

            core_copy(j).wait_send()
            rsc_copy(j).wait_send()
            for d in range(1, halves):
                x_copy(j, d).wait_send()
                fwd_copy(j, d).wait_send()
                rsx_copy(j, d).wait_send()

        when(j > 0, far)

    steps(drain)
    sh_core_copy().wait_send()
    for d in range(1, halves):
        sh_x_copy(d).wait_send()
    result.wait()


def wide_local(
    tokens,
    norm_gain,
    expert_ids,
    route_weights,
    gate_weight,
    up_weight,
    down_weight,
    shared_gate,
    shared_up,
    shared_down,
):
    tok, width = tokens.shape
    chosen = expert_ids.shape[1]
    n = lax.axis_size("ep")
    n_tp = lax.axis_size("tp")
    local_experts, _, ff = gate_weight.shape
    experts = n * local_experts
    cap = round_up((3 * tok * chosen + 2 * experts - 1) // (2 * experts), 16)
    share = width // n_tp
    halves = n_tp // 2
    chunk = local_experts * cap
    others = max(halves - 1, 1)
    hbm = pl.BlockSpec(memory_space=pltpu.HBM)
    dma = pltpu.SemaphoreType.DMA
    body = functools.partial(wide_kernel, n, n_tp, experts, cap)
    return pl.pallas_call(
        body,
        out_shape=jax.ShapeDtypeStruct((tok, share), BF16),
        in_specs=[hbm] * 10,
        out_specs=pl.BlockSpec(memory_space=pl.ANY),
        scratch_shapes=[
            pltpu.VMEM((tok, width), BF16),
            pltpu.VMEM((width,), BF16),
            pltpu.VMEM((chosen, tok), jnp.int32),
            pltpu.VMEM((chosen, tok), F32),
            pltpu.VMEM((tok, share), BF16),
            pltpu.VMEM((local_experts, width, 2 * ff), BF16),
            pltpu.VMEM((local_experts, ff, width), BF16),
            pltpu.VMEM((width, 2 * ff), BF16),
            pltpu.VMEM((ff, width), BF16),
            pltpu.VMEM((tok, width), BF16),
            pltpu.VMEM((round_up(experts, 128), tok), F32),
            pltpu.VMEM((chosen, tok, n * chunk), BF16),
            pltpu.VMEM((n, chunk, share), BF16),
            pltpu.VMEM((n, n_tp, chunk, share), BF16),
            pltpu.VMEM((n, 2, halves, chunk, share), BF16),
            pltpu.VMEM((n, halves, chunk, share), BF16),
            pltpu.VMEM((n, others, chunk, share), BF16),
            pltpu.VMEM((n, others, chunk, share), BF16),
            pltpu.VMEM((n, chunk, share), BF16),
            pltpu.VMEM((n, chunk, share), BF16),
            pltpu.VMEM((2, halves, tok, share), BF16),
            pltpu.VMEM((halves, tok, share), BF16),
            pltpu.VMEM((others, tok, share), BF16),
            pltpu.VMEM((others, tok, share), BF16),
            dma((4,)),
            dma((6,)),
            dma((n,)),
            dma((n,)),
            dma((n,)),
            dma((n,)),
            dma((n, others)),
            dma((n, others)),
            dma((n, others)),
            dma((n, others)),
            dma((n,)),
            dma((n,)),
            dma((n, others)),
            dma((n, others)),
            dma((n,)),
            dma((n,)),
            dma((halves,)),
            dma((halves,)),
        ],
        compiler_params=pltpu.CompilerParams(
            collective_id=0, has_side_effects=True, vmem_limit_bytes=67043328 - 3 * tok * share
        ),
        name="moe",
    )(
        tokens,
        norm_gain,
        expert_ids.T,
        route_weights.T,
        gate_weight,
        up_weight,
        down_weight,
        shared_gate,
        shared_up,
        shared_down,
    )


NEAR_Y, NEAR_Z, FAR_A, FAR_B = range(4)
ORDER = (
    ("arrive", FAR_A),
    ("shared", 1),
    ("arrive", NEAR_Z),
    ("arrive", NEAR_Y),
    ("arrive", FAR_B),
    ("crossed", FAR_A),
    ("hidden", NEAR_Z),
    ("hidden", FAR_A),
    ("hidden", NEAR_Y),
    ("crossed", FAR_B),
    ("hidden", FAR_B),
    ("down", NEAR_Z),
    ("down", FAR_A),
    ("down", NEAR_Y),
    ("down", FAR_B),
    ("shared", 2),
    ("add", NEAR_Z),
    ("add", NEAR_Y),
    ("add", FAR_A),
    ("add", FAR_B),
)


def paired_kernel(
    n,
    n_tp,
    cap,
    tokens_ref,
    gain_ref,
    ids_ref,
    rw_ref,
    wg_ref,
    wu_ref,
    wd_ref,
    sg_ref,
    su_ref,
    sd_ref,
    out_ref,
    tokens,
    gain,
    ids_v,
    rw_v,
    w_in,
    w_dn,
    sw_in,
    sw_out,
    normed,
    rank_t,
    cols,
    picks,
    send,
    rows,
    hid,
    back_out,
    back_in,
    acc,
    sh_terms,
    sh_core_in,
    sh_x_out,
    sh_x_in,
    in_sem,
    w_sem,
    a2a_s,
    a2a_r,
    core_s,
    core_r,
    x_s,
    x_r,
    wd_s,
    wd_r,
    hid_s,
    hid_r,
    ret_s,
    ret_r,
    sh_s,
    sh_r,
):
    tok, width = tokens_ref.shape
    share = width // n_tp
    ff = wg_ref.shape[2]
    chosen = ids_ref.shape[0]
    half, pair = n // 2, n // 4
    me = lax.axis_index("ep")
    tp = lax.axis_index("tp")
    hi, lo = tp // 2, tp % 2
    partner = hi * 2 + 1 - lo
    opposite = (1 - hi) * 2 + lo

    def peer(q):
        total, bit = 0, 1
        while bit < n:
            total = total + ((me // bit + q // bit) % 2) * bit
            bit *= 2
        return total

    def members(g):
        return [q for q in range(g * pair, (g + 1) * pair)]

    def away(g):
        return [q for q in members(g) if q > 0]

    def sibling(d):
        return (hi + d // 2) % 2 * 2 + (lo + d % 2) % 2

    firsts = [
        pltpu.make_async_copy(tokens_ref, tokens, in_sem.at[0]),
        pltpu.make_async_copy(gain_ref, gain, in_sem.at[1]),
        pltpu.make_async_copy(ids_ref, ids_v, in_sem.at[2]),
        pltpu.make_async_copy(rw_ref, rw_v, in_sem.at[3]),
    ]
    for load in firsts:
        load.start()

    barrier = pltpu.get_barrier_semaphore()
    for q in range(n - 1, 0, -1):
        pl.semaphore_signal(barrier, inc=1, device_id=(peer(q), tp), device_id_type=MESH)
    for d in range(1, n_tp):
        pl.semaphore_signal(barrier, inc=1, device_id=(me, sibling(d)), device_id_type=MESH)

    def features(t):
        return pl.ds(pl.multiple_of(t * share, 128), share)

    loads = [
        pltpu.make_async_copy(sg_ref, sw_in.at[:, pl.ds(0, ff)], w_sem.at[0]),
        pltpu.make_async_copy(su_ref, sw_in.at[:, pl.ds(ff, ff)], w_sem.at[1]),
        pltpu.make_async_copy(sd_ref, sw_out, w_sem.at[2]),
        pltpu.make_async_copy(wg_ref.at[0], w_in.at[:, pl.ds(0, ff)], w_sem.at[3]),
        pltpu.make_async_copy(wu_ref.at[0], w_in.at[:, pl.ds(ff, ff)], w_sem.at[4]),
        pltpu.make_async_copy(wd_ref.at[0, :, features(tp)], w_dn.at[tp], w_sem.at[5]),
    ]
    for load in loads:
        load.start()

    firsts[2].wait()
    firsts[3].wait()
    lanes = rank_t.shape[0]
    ids = [ids_v[k : k + 1, :] for k in range(chosen)]
    weights = [rw_v[k : k + 1, :] for k in range(chosen)]
    expert = lax.broadcasted_iota(jnp.int32, (lanes, tok), 0)
    named = ids[0] == expert
    for k in range(1, chosen):
        named = named | (ids[k] == expert)
    earlier = lax.broadcasted_iota(jnp.int32, (tok, tok), 0) < lax.broadcasted_iota(
        jnp.int32, (tok, tok), 1
    )
    rank = jnp.dot(
        jnp.where(named, 1.0, 0.0).astype(BF16),
        jnp.where(earlier, 1.0, 0.0).astype(BF16),
        preferred_element_type=F32,
    )
    rank_t[...] = jnp.where(named, rank, -1.0)

    firsts[0].wait()
    firsts[1].wait()
    values = tokens[...].astype(F32)
    scale = lax.rsqrt(jnp.mean(values * values, axis=-1, keepdims=True) + norm_eps)
    normed[...] = (values * scale * gain[...].astype(F32).reshape(1, width)).astype(BF16)

    slot_row = lax.broadcasted_iota(jnp.int32, (cap, tok), 0).astype(F32)

    def pick_rows(q):
        line = rank_t[pl.ds(peer(q), 1), :]
        return jnp.where(slot_row == line, 1.0, 0.0).astype(BF16)

    def a2a(q, outgoing=True):
        p = peer(q)
        owner = me if outgoing else p
        if q // pair < FAR_A:
            src, dst = send.at[q], rows.at[owner, lo]
        else:
            src, dst = send.at[q, 0], rows.at[owner, lo, hi]
        return pltpu.make_async_remote_copy(
            src_ref=src,
            dst_ref=dst,
            send_sem=a2a_s.at[q],
            recv_sem=a2a_r.at[owner],
            device_id=(p, tp),
            device_id_type=MESH,
        )

    def weight_copy(d, outgoing=True):
        t = sibling(d)
        return pltpu.make_async_remote_copy(
            src_ref=wd_ref.at[0, :, features(t)],
            dst_ref=w_dn.at[tp if outgoing else t],
            send_sem=wd_s.at[d],
            recv_sem=wd_r.at[d],
            device_id=(me, t),
            device_id_type=MESH,
        )

    def fill(g):
        targets = away(g)
        if not targets:
            return
        pick = jnp.concatenate([pick_rows(q) for q in targets], axis=0)
        for h in range(2) if g < FAR_A else (0,):
            t = h * 2 + lo if g < FAR_A else tp
            part = jnp.dot(
                pick, normed[:, features(t)], preferred_element_type=F32
            ).astype(BF16)
            for i, q in enumerate(targets):
                send[q, h] = part[i * cap : (i + 1) * cap]

    def launch(g):
        for q in away(g):
            a2a(q).start()

    def core_copy(q):
        block = rows.at[peer(q), lo]
        return pltpu.make_async_remote_copy(
            src_ref=block,
            dst_ref=block,
            send_sem=core_s.at[q],
            recv_sem=core_r.at[q],
            device_id=(me, partner),
            device_id_type=MESH,
        )

    def core_in(q):
        block = rows.at[peer(q), 1 - lo]
        return pltpu.make_async_remote_copy(
            src_ref=block,
            dst_ref=block,
            send_sem=core_s.at[q],
            recv_sem=core_r.at[q],
            device_id=(me, partner),
            device_id_type=MESH,
        )

    def x_copy(q, outgoing=True):
        block = rows.at[peer(q), lo, hi if outgoing else 1 - hi]
        return pltpu.make_async_remote_copy(
            src_ref=block,
            dst_ref=block,
            send_sem=x_s.at[q],
            recv_sem=x_r.at[q],
            device_id=(me, opposite),
            device_id_type=MESH,
        )

    def hid_copy(g, d, outgoing=True):
        t = sibling(d)
        return pltpu.make_async_remote_copy(
            src_ref=hid.at[g, tp],
            dst_ref=hid.at[g, tp if outgoing else t],
            send_sem=hid_s.at[g, d],
            recv_sem=hid_r.at[g, d],
            device_id=(me, t),
            device_id_type=MESH,
        )

    def ret_copy(q, outgoing=True):
        p = peer(q)
        owner = me if outgoing else p
        return pltpu.make_async_remote_copy(
            src_ref=back_out.at[q],
            dst_ref=back_in.at[owner],
            send_sem=ret_s.at[q],
            recv_sem=ret_r.at[owner],
            device_id=(p, tp),
            device_id_type=MESH,
        )

    def sh_core_copy():
        return pltpu.make_async_remote_copy(
            src_ref=sh_terms.at[1 - lo],
            dst_ref=sh_core_in,
            send_sem=sh_s.at[0],
            recv_sem=sh_r.at[0],
            device_id=(me, partner),
            device_id_type=MESH,
        )

    def sh_x_copy():
        return pltpu.make_async_remote_copy(
            src_ref=sh_x_out,
            dst_ref=sh_x_in,
            send_sem=sh_s.at[1],
            recv_sem=sh_r.at[1],
            device_id=(me, opposite),
            device_id_type=MESH,
        )

    def hidden_of(mixed):
        gate, up = mixed[:, :ff], mixed[:, ff:]
        return (gate / (1.0 + jnp.exp(-gate)) * up).astype(BF16)

    def make_picks():
        lines = [rank_t[pl.ds(peer(q), 1), :] for q in range(n)]
        for q in range(n):
            p = peer(q)
            weight = jnp.zeros((1, tok), F32)
            for k in range(chosen):
                weight = weight + jnp.where(ids[k] == p, weights[k], 0.0)
            lines.append(weight)
        at_row = lax.broadcasted_iota(jnp.int32, (tok, tok), 0)
        table = jnp.zeros((tok, tok), F32)
        for index, line in enumerate(lines):
            table = jnp.where(at_row == index, line, table)
        table = table.T
        cols[...] = table
        slot = lax.broadcasted_iota(jnp.int32, (tok, cap), 1).astype(F32)
        for q in range(n):
            picks[q] = jnp.where(slot == table[:, q : q + 1], 1.0, 0.0).astype(BF16)

    fill(FAR_A)
    fill(FAR_B)
    pl.semaphore_wait(barrier, n - 1 + n_tp - 1)
    launch(FAR_A)
    launch(FAR_B)
    for g in (NEAR_Z, NEAR_Y):
        fill(g)
        launch(g)
    for d in (2, 3, 1):
        weight_copy(d).start()

    for load in loads[:3]:
        load.wait()
    sh_hidden = hidden_of(jnp.dot(normed[...], sw_in[...], preferred_element_type=F32))
    for t in range(n_tp):
        sh_terms[t % 2, t // 2] = jnp.dot(
            sh_hidden, sw_out[:, pl.ds(t * share, share)], preferred_element_type=F32
        ).astype(BF16)
    sh_core_copy().start()
    own = pick_rows(0)
    for t in range(n_tp):
        rows[me, t % 2, t // 2] = jnp.dot(
            own, normed[:, pl.ds(t * share, share)], preferred_element_type=F32
        ).astype(BF16)
    make_picks()
    for load in loads[3:5]:
        load.wait()

    def shared(stage):
        if stage == 1:
            sh_core_copy().wait_recv()
            sh_x_out[...] = (
                sh_terms[lo, 1 - hi].astype(F32) + sh_core_in[1 - hi].astype(F32)
            ).astype(BF16)
            sh_x_copy().start()
        else:
            total = sh_terms[lo, hi].astype(F32) + sh_core_in[hi].astype(F32)
            sh_x_copy().wait_recv()
            acc[...] = total + sh_x_in[...].astype(F32)

    def arrive(g):
        for q in away(g):
            a2a(q, False).wait_recv()
            if g < FAR_A:
                core_copy(q).start()
            else:
                x_copy(q).start()

    def crossed(g):
        for q in away(g):
            x_copy(q, False).wait_recv()
            core_copy(q).start()

    def hidden(g):
        for q in away(g):
            core_in(q).wait_recv()
        total = jnp.zeros((pair * cap, 2 * ff), F32)
        for t in range(n_tp):
            block = jnp.concatenate(
                [rows[peer(q), t % 2, t // 2] for q in members(g)], axis=0
            )
            total = total + jnp.dot(
                block, w_in[pl.ds(t * share, share), :], preferred_element_type=F32
            )
        hid[g, tp] = hidden_of(total)
        for d in (2, 3, 1):
            hid_copy(g, d).start()

    placed = []

    def down(g):
        if not placed:
            loads[5].wait()
            for d in range(1, n_tp):
                weight_copy(d, False).wait_recv()
            placed.append(True)
        for d in range(1, n_tp):
            hid_copy(g, d, False).wait_recv()
        block = jnp.concatenate([hid[g, t] for t in range(n_tp)], axis=1)
        total = jnp.dot(
            block, w_dn[...].reshape(n_tp * ff, share), preferred_element_type=F32
        ).astype(BF16)
        for i, q in enumerate(members(g)):
            part = total[i * cap : (i + 1) * cap]
            if q == 0:
                back_in[me] = part
            else:
                back_out[q] = part
                ret_copy(q).start()

    def add(g):
        total = acc[...]
        for q in members(g):
            if q > 0:
                ret_copy(q, False).wait_recv()
            total = total + cols[:, n + q : n + q + 1] * jnp.dot(
                picks[q], back_in[peer(q)], preferred_element_type=F32
            )
        if g == ORDER[-1][1]:
            out_ref[...] = total.astype(BF16)
        else:
            acc[...] = total

    steps = dict(
        shared=shared, arrive=arrive, crossed=crossed, hidden=hidden, down=down, add=add
    )
    for name, which in ORDER:
        steps[name](which)

    for q in range(1, n):
        a2a(q).wait_send()
        core_copy(q).wait_send()
        ret_copy(q).wait_send()
        if q // pair >= FAR_A:
            x_copy(q).wait_send()
    for g in range(4):
        for d in range(1, n_tp):
            hid_copy(g, d).wait_send()
    for d in range(1, n_tp):
        weight_copy(d).wait_send()
    sh_core_copy().wait_send()
    sh_x_copy().wait_send()


def local(
    tokens,
    norm_gain,
    expert_ids,
    route_weights,
    gate_weight,
    up_weight,
    down_weight,
    shared_gate,
    shared_up,
    shared_down,
):
    tok, width = tokens.shape
    chosen = expert_ids.shape[1]
    n = lax.axis_size("ep")
    n_tp = lax.axis_size("tp")
    local_experts, _, ff = gate_weight.shape
    fits = n & (n - 1) == 0 and 4 <= n <= 8 and n_tp == 4 and local_experts == 1
    if not fits:
        return wide_local(
            tokens,
            norm_gain,
            expert_ids,
            route_weights,
            gate_weight,
            up_weight,
            down_weight,
            shared_gate,
            shared_up,
            shared_down,
        )
    cap = round_up((3 * tok * chosen + 2 * n - 1) // (2 * n), 16)
    share = width // n_tp
    pair = n // 4
    hbm = pl.BlockSpec(memory_space=pltpu.HBM)
    dma = pltpu.SemaphoreType.DMA
    return pl.pallas_call(
        functools.partial(paired_kernel, n, n_tp, cap),
        out_shape=pltpu.VMEM((tok, share), BF16),
        in_specs=[hbm] * 10,
        out_specs=pl.BlockSpec(memory_space=pltpu.VMEM),
        scratch_shapes=[
            pltpu.VMEM((tok, width), BF16),
            pltpu.VMEM((width,), BF16),
            pltpu.VMEM((chosen, tok), jnp.int32),
            pltpu.VMEM((chosen, tok), F32),
            pltpu.VMEM((width, 2 * ff), BF16),
            pltpu.VMEM((n_tp, ff, share), BF16),
            pltpu.VMEM((width, 2 * ff), BF16),
            pltpu.VMEM((ff, width), BF16),
            pltpu.VMEM((tok, width), BF16),
            pltpu.VMEM((round_up(n, 128), tok), F32),
            pltpu.VMEM((tok, tok), F32),
            pltpu.VMEM((n, tok, cap), BF16),
            pltpu.VMEM((n, 2, cap, share), BF16),
            pltpu.VMEM((n, 2, 2, cap, share), BF16),
            pltpu.VMEM((4, n_tp, pair * cap, ff), BF16),
            pltpu.VMEM((n, cap, share), BF16),
            pltpu.VMEM((n, cap, share), BF16),
            pltpu.VMEM((tok, share), F32),
            pltpu.VMEM((2, 2, tok, share), BF16),
            pltpu.VMEM((2, tok, share), BF16),
            pltpu.VMEM((tok, share), BF16),
            pltpu.VMEM((tok, share), BF16),
            dma((4,)),
            dma((6,)),
            dma((n,)),
            dma((n,)),
            dma((n,)),
            dma((n,)),
            dma((n,)),
            dma((n,)),
            dma((n_tp,)),
            dma((n_tp,)),
            dma((4, n_tp)),
            dma((4, n_tp)),
            dma((n,)),
            dma((n,)),
            dma((2,)),
            dma((2,)),
        ],
        compiler_params=pltpu.CompilerParams(
            collective_id=0, has_side_effects=True, vmem_limit_bytes=60000000
        ),
        name="moe",
    )(
        tokens,
        norm_gain,
        expert_ids.T,
        route_weights.T,
        gate_weight,
        up_weight,
        down_weight,
        shared_gate,
        shared_up,
        shared_down,
    )


def solution(mesh):
    in_specs = (
        P("ep", None),
        P(),
        P("ep", None),
        P("ep", None),
        P("ep", None, "tp"),
        P("ep", None, "tp"),
        P("ep", "tp", None),
        P(None, "tp"),
        P(None, "tp"),
        P("tp", None),
    )
    out_specs = P("ep", "tp")
    return jax.shard_map(local, mesh=mesh, in_specs=in_specs, out_specs=out_specs, check_vma=False)
```

```python
import functools

import jax
import jax.numpy as jnp
from jax import lax
from jax.experimental import pallas as pl
from jax.experimental.pallas import tpu as pltpu
from jax.sharding import PartitionSpec as P

norm_eps = 1e-06
MESH = pl.DeviceIdType.MESH
ARRIVE, SPACING, SHARED = 2.7, 1.3, 2.0
LATENCY = (0.0, 4.0, 1.5, 2.5, 4.0)
F32, BF16 = jnp.float32, jnp.bfloat16


def round_up(value, unit):
    return (value + unit - 1) // unit * unit


def wide_kernel(
    n,
    n_tp,
    experts,
    cap,
    tokens_ref,
    gain_ref,
    ids_ref,
    rw_ref,
    wg_ref,
    wu_ref,
    wd_ref,
    sg_ref,
    su_ref,
    sd_ref,
    out_ref,
    tokens,
    gain,
    ids_v,
    rw_v,
    out_v,
    w_in,
    w_out,
    sw_in,
    sw_out,
    normed,
    rank_t,
    picks,
    send,
    rows,
    terms,
    core_in,
    x_out,
    x_in,
    back_out,
    back_in,
    sh_terms,
    sh_core_in,
    sh_x_out,
    sh_x_in,
    in_sem,
    w_sem,
    a2a_s,
    a2a_r,
    core_s,
    core_r,
    x_s,
    x_r,
    fwd_s,
    fwd_r,
    rsc_s,
    rsc_r,
    rsx_s,
    rsx_r,
    ret_s,
    ret_r,
    sh_s,
    sh_r,
):
    tok, width = tokens_ref.shape
    share = width // n_tp
    local_experts, _, ff = wg_ref.shape
    chosen = ids_ref.shape[0]
    halves = n_tp // 2
    me = lax.axis_index("ep")
    tp = lax.axis_index("tp")
    hi, lo = tp // 2, tp % 2
    partner = hi * 2 + 1 - lo

    def across(d):
        return (hi + d) % halves

    def steps(body):
        if n <= 8:
            for j in range(n):
                body(j)
        else:

            def one(j, carry):
                body(j)
                return carry

            lax.fori_loop(0, n, one, 0)

    def mirror(j):
        total, bit = 0, 1
        while bit < n:
            total = total + ((me // bit + j // bit) % 2) * bit
            bit *= 2
        return total

    even = n & (n - 1) == 0

    def source(j):
        return mirror(j) if even else (me - j + n) % n

    def target(j):
        return mirror(j) if even else (me + j) % n

    def when(cond, body):
        if isinstance(cond, bool):
            if cond:
                body()
        else:
            pl.when(cond)(body)

    firsts = [
        pltpu.make_async_copy(tokens_ref, tokens, in_sem.at[0]),
        pltpu.make_async_copy(gain_ref, gain, in_sem.at[1]),
        pltpu.make_async_copy(ids_ref, ids_v, in_sem.at[2]),
        pltpu.make_async_copy(rw_ref, rw_v, in_sem.at[3]),
    ]
    for load in firsts:
        load.start()

    barrier = pltpu.get_barrier_semaphore()

    def greet(j):
        def go():
            pl.semaphore_signal(barrier, inc=1, device_id=(target(j), tp), device_id_type=MESH)

        when(j > 0, go)

    steps(greet)
    pl.semaphore_signal(barrier, inc=1, device_id=(me, partner), device_id_type=MESH)
    for d in range(1, halves):
        pl.semaphore_signal(
            barrier, inc=1, device_id=(me, across(d) * 2 + lo), device_id_type=MESH
        )

    loads = [
        pltpu.make_async_copy(sg_ref, sw_in.at[:, pl.ds(0, ff)], w_sem.at[0]),
        pltpu.make_async_copy(su_ref, sw_in.at[:, pl.ds(ff, ff)], w_sem.at[1]),
        pltpu.make_async_copy(sd_ref, sw_out, w_sem.at[2]),
        pltpu.make_async_copy(wg_ref, w_in.at[:, :, pl.ds(0, ff)], w_sem.at[3]),
        pltpu.make_async_copy(wu_ref, w_in.at[:, :, pl.ds(ff, ff)], w_sem.at[4]),
        pltpu.make_async_copy(wd_ref, w_out, w_sem.at[5]),
    ]
    for load in loads:
        load.start()

    firsts[2].wait()
    firsts[3].wait()
    lanes = rank_t.shape[0]
    ids = [ids_v[k : k + 1, :] for k in range(chosen)]
    weights = [rw_v[k : k + 1, :] for k in range(chosen)]
    expert = lax.broadcasted_iota(jnp.int32, (lanes, tok), 0)
    named = ids[0] == expert
    for k in range(1, chosen):
        named = named | (ids[k] == expert)
    earlier = lax.broadcasted_iota(jnp.int32, (tok, tok), 0) < lax.broadcasted_iota(
        jnp.int32, (tok, tok), 1
    )
    rank = jnp.dot(
        jnp.where(named, 1.0, 0.0).astype(BF16),
        jnp.where(earlier, 1.0, 0.0).astype(BF16),
        preferred_element_type=F32,
    )
    rank_t[...] = jnp.where(named, rank, -1.0)

    firsts[0].wait()
    firsts[1].wait()
    values = tokens[...].astype(F32)
    scale = lax.rsqrt(jnp.mean(values * values, axis=-1, keepdims=True) + norm_eps)
    normed[...] = (values * scale * gain[...].astype(F32).reshape(1, width)).astype(BF16)

    chunk = local_experts * cap
    slot_row = lax.broadcasted_iota(jnp.int32, (cap, tok), 0).astype(F32)
    column = pl.ds(pl.multiple_of(tp * share, 128), share)

    def dispatch(j, features):
        p = target(j)
        parts = []
        for le in range(local_experts):
            line = rank_t[pl.ds(p * local_experts + le, 1), :]
            pick = jnp.where(slot_row == line, 1.0, 0.0).astype(BF16)
            parts.append(
                jnp.dot(pick, normed[:, features], preferred_element_type=F32).astype(BF16)
            )
        return parts

    def a2a(j):
        return pltpu.make_async_remote_copy(
            src_ref=send.at[j],
            dst_ref=rows.at[me, tp],
            send_sem=a2a_s.at[j],
            recv_sem=a2a_r.at[me],
            device_id=(target(j), tp),
            device_id_type=MESH,
        )

    def a2a_in(j):
        s = source(j)
        return pltpu.make_async_remote_copy(
            src_ref=send.at[j],
            dst_ref=rows.at[s, tp],
            send_sem=a2a_s.at[j],
            recv_sem=a2a_r.at[s],
            device_id=(target(j), tp),
            device_id_type=MESH,
        )

    pl.semaphore_wait(barrier, (n - 1) + 1 + (halves - 1))

    def dispatch_and_send(j):
        def go():
            for le, part in enumerate(dispatch(j, column)):
                send[j, pl.ds(le * cap, cap), :] = part
            a2a(j).start()

        when(j > 0, go)

    steps(dispatch_and_send)

    def core_copy(j):
        s = source(j)
        return pltpu.make_async_remote_copy(
            src_ref=rows.at[s, tp],
            dst_ref=rows.at[s, tp],
            send_sem=core_s.at[j],
            recv_sem=core_r.at[j],
            device_id=(me, partner),
            device_id_type=MESH,
        )

    def x_copy(j, d):
        s = source(j)
        return pltpu.make_async_remote_copy(
            src_ref=rows.at[s, tp],
            dst_ref=rows.at[s, tp],
            send_sem=x_s.at[j, d - 1],
            recv_sem=x_r.at[j, d - 1],
            device_id=(me, across(d) * 2 + lo),
            device_id_type=MESH,
        )

    def fwd_copy(j, d):
        s = source(j)
        held = across(halves - d) * 2 + lo
        return pltpu.make_async_remote_copy(
            src_ref=rows.at[s, held],
            dst_ref=rows.at[s, held],
            send_sem=fwd_s.at[j, d - 1],
            recv_sem=fwd_r.at[j, d - 1],
            device_id=(me, partner),
            device_id_type=MESH,
        )

    def stage_a(j):
        a2a_in(j).wait_recv()
        for d in range(1, halves):
            x_copy(j, d).start()
        core_copy(j).start()

    def stage_b(j):
        for d in range(1, halves):
            x_copy(j, d).wait_recv()
            fwd_copy(j, d).start()

    def rsc_copy(j):
        return pltpu.make_async_remote_copy(
            src_ref=terms.at[j, 1 - lo],
            dst_ref=core_in.at[j],
            send_sem=rsc_s.at[j],
            recv_sem=rsc_r.at[j],
            device_id=(me, partner),
            device_id_type=MESH,
        )

    def rsx_copy(j, d):
        return pltpu.make_async_remote_copy(
            src_ref=x_out.at[j, d - 1],
            dst_ref=x_in.at[j, d - 1],
            send_sem=rsx_s.at[j, d - 1],
            recv_sem=rsx_r.at[j, d - 1],
            device_id=(me, across(d) * 2 + lo),
            device_id_type=MESH,
        )

    def ret_copy(j):
        return pltpu.make_async_remote_copy(
            src_ref=back_out.at[j],
            dst_ref=back_in.at[me],
            send_sem=ret_s.at[j],
            recv_sem=ret_r.at[me],
            device_id=(source(j), tp),
            device_id_type=MESH,
        )

    def ret_in(j):
        g = target(j)
        return pltpu.make_async_remote_copy(
            src_ref=back_out.at[j],
            dst_ref=back_in.at[g],
            send_sem=ret_s.at[j],
            recv_sem=ret_r.at[g],
            device_id=(source(j), tp),
            device_id_type=MESH,
        )

    def hidden_of(mixed):
        gate, up = mixed[:, :ff], mixed[:, ff:]
        return (gate / (1.0 + jnp.exp(-gate)) * up).astype(BF16)

    def expert_hidden(s, le):
        total = jnp.zeros((cap, 2 * ff), F32)
        for t in range(n_tp):
            total = total + jnp.dot(
                rows[s, t, pl.ds(le * cap, cap), :],
                w_in[le, pl.ds(t * share, share), :],
                preferred_element_type=F32,
            )
        return hidden_of(total)

    def stage_c(j):
        core_copy(j).wait_recv()
        for d in range(1, halves):
            fwd_copy(j, d).wait_recv()
        for le in range(local_experts):
            hidden = expert_hidden(source(j), le)
            for t in range(n_tp):
                terms[j, t % 2, t // 2, pl.ds(le * cap, cap), :] = jnp.dot(
                    hidden,
                    w_out[le, :, pl.ds(t * share, share)],
                    preferred_element_type=F32,
                ).astype(BF16)
        rsc_copy(j).start()

    def stage_d(j):
        rsc_copy(j).wait_recv()
        for d in range(1, halves):
            h = across(d)
            x_out[j, d - 1] = (
                terms[j, lo, h].astype(F32) + core_in[j, h].astype(F32)
            ).astype(BF16)
            rsx_copy(j, d).start()

    def stage_e(j):
        total = terms[j, lo, hi].astype(F32) + core_in[j, hi].astype(F32)
        for d in range(1, halves):
            rsx_copy(j, d).wait_recv()
            total = total + x_in[j, d - 1].astype(F32)
        back_out[j] = total.astype(BF16)

        ret_copy(j).start()

    def sh_core_copy():
        return pltpu.make_async_remote_copy(
            src_ref=sh_terms.at[1 - lo],
            dst_ref=sh_core_in,
            send_sem=sh_s.at[0],
            recv_sem=sh_r.at[0],
            device_id=(me, partner),
            device_id_type=MESH,
        )

    def sh_x_copy(d):
        return pltpu.make_async_remote_copy(
            src_ref=sh_x_out.at[d - 1],
            dst_ref=sh_x_in.at[d - 1],
            send_sem=sh_s.at[d],
            recv_sem=sh_r.at[d],
            device_id=(me, across(d) * 2 + lo),
            device_id_type=MESH,
        )

    def make_picks():
        slots = n * chunk
        place = rank + (expert * cap).astype(F32)
        lines = [
            jnp.sum(jnp.where(ids[k] == expert, place, 0.0), axis=0, keepdims=True)
            for k in range(chosen)
        ] + weights
        for le in range(local_experts):
            mine = me * local_experts + le
            lines.append(rank_t[pl.ds(mine, 1), :])
            weight = jnp.zeros((1, tok), F32)
            for k in range(chosen):
                weight = weight + jnp.where(ids[k] == mine, weights[k], 0.0)
            lines.append(weight)
        at_row = lax.broadcasted_iota(jnp.int32, (tok, tok), 0)
        table = jnp.zeros((tok, tok), F32)
        for index, line in enumerate(lines):
            table = jnp.where(at_row == index, line, table)
        table = table.T
        spot = lax.broadcasted_iota(jnp.int32, (tok, slots), 1).astype(F32)
        for k in range(chosen):
            picks[k] = jnp.where(spot == table[:, k : k + 1], 1.0, 0.0).astype(BF16)
        return table

    def shared_first():
        for load in loads[:3]:
            load.wait()
        hidden = hidden_of(jnp.dot(normed[...], sw_in[...], preferred_element_type=F32))
        slot = lax.broadcasted_iota(jnp.int32, (tok, cap), 1).astype(F32)
        table = make_picks()
        for load in loads[3:]:
            load.wait()
        own = []
        for le in range(local_experts):
            for t in range(n_tp):
                features = pl.ds(t * share, share)
                rows[me, t, pl.ds(le * cap, cap), :] = dispatch(0, features)[le]
            own.append(expert_hidden(me, le))
        for t in range(n_tp):
            features = pl.ds(t * share, share)
            total = jnp.dot(hidden, sw_out[:, features], preferred_element_type=F32)
            for le in range(local_experts):
                at = 2 * chosen + 2 * le
                pick = jnp.where(slot == table[:, at : at + 1], 1.0, 0.0).astype(BF16)
                term = jnp.dot(
                    own[le], w_out[le, :, features], preferred_element_type=F32
                ).astype(BF16)
                total = total + table[:, at + 1 : at + 2] * jnp.dot(
                    pick, term, preferred_element_type=F32
                )
            sh_terms[t % 2, t // 2] = total.astype(BF16)
        sh_core_copy().start()
        return [table[:, chosen + k : chosen + k + 1] for k in range(chosen)]

    def shared_second():
        sh_core_copy().wait_recv()
        for d in range(1, halves):
            h = across(d)
            sh_x_out[d - 1] = (sh_terms[lo, h].astype(F32) + sh_core_in[h].astype(F32)).astype(
                BF16
            )
            sh_x_copy(d).start()

    back_in[me] = jnp.zeros((chunk, share), BF16)
    route = shared_first()

    stages = (stage_a, stage_b, stage_c, stage_d, stage_e)

    if n <= 8:
        order = []
        for j in range(1, n):
            at = ARRIVE + SPACING * (j - 1)
            for index, stage in enumerate(stages):
                at += LATENCY[index]
                order.append((at, index, j))
        order.append((SHARED, -1, 0))
        for _, index, j in sorted(order):
            if index < 0:
                shared_second()
            else:
                stages[index](j)
    else:
        shared_second()
        lags = (0, 2, 3, 4, 6)

        def one(i, carry):
            for lag, stage in zip(lags, stages):
                pl.when((i - lag >= 1) & (i - lag < n))(functools.partial(stage, i - lag))
            return carry

        lax.fori_loop(1, n + lags[-1], one, 0)

    total = sh_terms[lo, hi].astype(F32) + sh_core_in[hi].astype(F32)
    for d in range(1, halves):
        sh_x_copy(d).wait_recv()
        total = total + sh_x_in[d - 1].astype(F32)

    steps(lambda j: when(j > 0, lambda: ret_in(j).wait_recv()))
    came = back_in[...].reshape(n * chunk, share)
    for k in range(chosen):
        total = total + route[k] * jnp.dot(
            picks[k], came, preferred_element_type=F32
        )
    out_v[...] = total.astype(BF16)
    result = pltpu.make_async_copy(out_v, out_ref, in_sem.at[0])
    result.start()

    def drain(j):
        def far():
            a2a(j).wait_send()
            ret_copy(j).wait_send()

            core_copy(j).wait_send()
            rsc_copy(j).wait_send()
            for d in range(1, halves):
                x_copy(j, d).wait_send()
                fwd_copy(j, d).wait_send()
                rsx_copy(j, d).wait_send()

        when(j > 0, far)

    steps(drain)
    sh_core_copy().wait_send()
    for d in range(1, halves):
        sh_x_copy(d).wait_send()
    result.wait()


def wide_local(
    tokens,
    norm_gain,
    expert_ids,
    route_weights,
    gate_weight,
    up_weight,
    down_weight,
    shared_gate,
    shared_up,
    shared_down,
):
    tok, width = tokens.shape
    chosen = expert_ids.shape[1]
    n = lax.axis_size("ep")
    n_tp = lax.axis_size("tp")
    local_experts, _, ff = gate_weight.shape
    experts = n * local_experts
    cap = round_up((3 * tok * chosen + 2 * experts - 1) // (2 * experts), 16)
    share = width // n_tp
    halves = n_tp // 2
    chunk = local_experts * cap
    others = max(halves - 1, 1)
    hbm = pl.BlockSpec(memory_space=pltpu.HBM)
    dma = pltpu.SemaphoreType.DMA
    body = functools.partial(wide_kernel, n, n_tp, experts, cap)
    return pl.pallas_call(
        body,
        out_shape=jax.ShapeDtypeStruct((tok, share), BF16),
        in_specs=[hbm] * 10,
        out_specs=pl.BlockSpec(memory_space=pl.ANY),
        scratch_shapes=[
            pltpu.VMEM((tok, width), BF16),
            pltpu.VMEM((width,), BF16),
            pltpu.VMEM((chosen, tok), jnp.int32),
            pltpu.VMEM((chosen, tok), F32),
            pltpu.VMEM((tok, share), BF16),
            pltpu.VMEM((local_experts, width, 2 * ff), BF16),
            pltpu.VMEM((local_experts, ff, width), BF16),
            pltpu.VMEM((width, 2 * ff), BF16),
            pltpu.VMEM((ff, width), BF16),
            pltpu.VMEM((tok, width), BF16),
            pltpu.VMEM((round_up(experts, 128), tok), F32),
            pltpu.VMEM((chosen, tok, n * chunk), BF16),
            pltpu.VMEM((n, chunk, share), BF16),
            pltpu.VMEM((n, n_tp, chunk, share), BF16),
            pltpu.VMEM((n, 2, halves, chunk, share), BF16),
            pltpu.VMEM((n, halves, chunk, share), BF16),
            pltpu.VMEM((n, others, chunk, share), BF16),
            pltpu.VMEM((n, others, chunk, share), BF16),
            pltpu.VMEM((n, chunk, share), BF16),
            pltpu.VMEM((n, chunk, share), BF16),
            pltpu.VMEM((2, halves, tok, share), BF16),
            pltpu.VMEM((halves, tok, share), BF16),
            pltpu.VMEM((others, tok, share), BF16),
            pltpu.VMEM((others, tok, share), BF16),
            dma((4,)),
            dma((6,)),
            dma((n,)),
            dma((n,)),
            dma((n,)),
            dma((n,)),
            dma((n, others)),
            dma((n, others)),
            dma((n, others)),
            dma((n, others)),
            dma((n,)),
            dma((n,)),
            dma((n, others)),
            dma((n, others)),
            dma((n,)),
            dma((n,)),
            dma((halves,)),
            dma((halves,)),
        ],
        compiler_params=pltpu.CompilerParams(
            collective_id=0, has_side_effects=True, vmem_limit_bytes=67043328 - 3 * tok * share
        ),
        name="moe",
    )(
        tokens,
        norm_gain,
        expert_ids.T,
        route_weights.T,
        gate_weight,
        up_weight,
        down_weight,
        shared_gate,
        shared_up,
        shared_down,
    )


NEAR_Z, NEAR_Y, FAR_A, FAR_B = range(4)
ORDER = (
    ("shared", 1),
    ("arrive", FAR_A),
    ("arrive", NEAR_Z),
    ("arrive", FAR_B),
    ("arrive", NEAR_Y),
    ("crossed", FAR_A),
    ("hidden", NEAR_Z),
    ("hidden", FAR_A),
    ("hidden", NEAR_Y),
    ("crossed", FAR_B),
    ("hidden", FAR_B),
    ("down", NEAR_Z),
    ("down", FAR_A),
    ("down", NEAR_Y),
    ("down", FAR_B),
    ("shared", 2),
    ("add", NEAR_Z),
    ("add", NEAR_Y),
    ("add", FAR_A),
    ("add", FAR_B),
)


def split(n):
    half, pair = n // 2, n // 4
    return [
        tuple(range(pair, half)),
        tuple(range(pair)),
        tuple(range(half, half + pair)),
        tuple(range(half + pair, n)),
    ]


def paired_kernel(
    n,
    n_tp,
    cap,
    tokens_ref,
    gain_ref,
    ids_ref,
    rw_ref,
    wg_ref,
    wu_ref,
    wd_ref,
    sg_ref,
    su_ref,
    sd_ref,
    out_ref,
    tokens,
    gain,
    ids_v,
    rw_v,
    w_in,
    w_dn,
    sw_in,
    sw_out,
    normed,
    rank_t,
    cols,
    picks,
    send,
    rows,
    hid,
    back_out,
    back_in,
    acc,
    sh_terms,
    sh_core_in,
    sh_x_out,
    sh_x_in,
    in_sem,
    w_sem,
    a2a_s,
    a2a_r,
    core_s,
    core_r,
    x_s,
    x_r,
    wd_s,
    wd_r,
    hid_s,
    hid_r,
    ret_s,
    ret_r,
    sh_s,
    sh_r,
):
    tok, width = tokens_ref.shape
    share = width // n_tp
    ff = wg_ref.shape[2]
    chosen = ids_ref.shape[0]
    half, pair = n // 2, n // 4
    groups = split(n)
    me = lax.axis_index("ep")
    tp = lax.axis_index("tp")
    hi, lo = tp // 2, tp % 2
    partner = hi * 2 + 1 - lo
    opposite = (1 - hi) * 2 + lo

    def peer(q):
        total, bit = 0, 1
        while bit < n:
            total = total + ((me // bit + q // bit) % 2) * bit
            bit *= 2
        return total

    def away(g):
        return [q for q in groups[g] if q > 0]

    def sibling(d):
        return (hi + d // 2) % 2 * 2 + (lo + d % 2) % 2

    firsts = [
        pltpu.make_async_copy(tokens_ref, tokens, in_sem.at[0]),
        pltpu.make_async_copy(gain_ref, gain, in_sem.at[1]),
        pltpu.make_async_copy(ids_ref, ids_v, in_sem.at[2]),
        pltpu.make_async_copy(rw_ref, rw_v, in_sem.at[3]),
    ]
    for load in firsts:
        load.start()

    barrier = pltpu.get_barrier_semaphore()
    for q in range(n - 1, 0, -1):
        pl.semaphore_signal(barrier, inc=1, device_id=(peer(q), tp), device_id_type=MESH)
    for d in range(1, n_tp):
        pl.semaphore_signal(barrier, inc=1, device_id=(me, sibling(d)), device_id_type=MESH)

    def features(t):
        return pl.ds(pl.multiple_of(t * share, 128), share)

    loads = [
        pltpu.make_async_copy(sg_ref, sw_in.at[:, pl.ds(0, ff)], w_sem.at[0]),
        pltpu.make_async_copy(su_ref, sw_in.at[:, pl.ds(ff, ff)], w_sem.at[1]),
        pltpu.make_async_copy(sd_ref, sw_out, w_sem.at[2]),
        pltpu.make_async_copy(wg_ref.at[0], w_in.at[:, pl.ds(0, ff)], w_sem.at[3]),
        pltpu.make_async_copy(wu_ref.at[0], w_in.at[:, pl.ds(ff, ff)], w_sem.at[4]),
        pltpu.make_async_copy(wd_ref.at[0, :, features(tp)], w_dn.at[tp], w_sem.at[5]),
    ]
    for load in loads:
        load.start()

    firsts[2].wait()
    firsts[3].wait()
    lanes = rank_t.shape[0]
    ids = [ids_v[k : k + 1, :] for k in range(chosen)]
    weights = [rw_v[k : k + 1, :] for k in range(chosen)]
    expert = lax.broadcasted_iota(jnp.int32, (lanes, tok), 0)
    named = ids[0] == expert
    for k in range(1, chosen):
        named = named | (ids[k] == expert)
    earlier = lax.broadcasted_iota(jnp.int32, (tok, tok), 0) < lax.broadcasted_iota(
        jnp.int32, (tok, tok), 1
    )
    rank = jnp.dot(
        jnp.where(named, 1.0, 0.0).astype(BF16),
        jnp.where(earlier, 1.0, 0.0).astype(BF16),
        preferred_element_type=F32,
    )
    rank_t[...] = jnp.where(named, rank, -1.0)

    firsts[0].wait()
    firsts[1].wait()
    values = tokens[...].astype(F32)
    scale = lax.rsqrt(jnp.mean(values * values, axis=-1, keepdims=True) + norm_eps)
    normed[...] = (values * scale * gain[...].astype(F32).reshape(1, width)).astype(BF16)

    slot_row = lax.broadcasted_iota(jnp.int32, (cap, tok), 0).astype(F32)

    def pick_rows(q):
        line = rank_t[pl.ds(peer(q), 1), :]
        return jnp.where(slot_row == line, 1.0, 0.0).astype(BF16)

    def a2a(q, outgoing=True):
        p = peer(q)
        owner = me if outgoing else p
        if q < half:
            src, dst = send.at[q], rows.at[owner, lo]
        else:
            src, dst = send.at[q, 0], rows.at[owner, lo, hi]
        return pltpu.make_async_remote_copy(
            src_ref=src,
            dst_ref=dst,
            send_sem=a2a_s.at[q],
            recv_sem=a2a_r.at[owner],
            device_id=(p, tp),
            device_id_type=MESH,
        )

    def weight_copy(d, outgoing=True):
        t = sibling(d)
        return pltpu.make_async_remote_copy(
            src_ref=wd_ref.at[0, :, features(t)],
            dst_ref=w_dn.at[tp if outgoing else t],
            send_sem=wd_s.at[d],
            recv_sem=wd_r.at[d],
            device_id=(me, t),
            device_id_type=MESH,
        )

    def fill(targets):
        near = targets[0] < half
        pick = jnp.concatenate([pick_rows(q) for q in targets], axis=0)
        for h in range(2) if near else (0,):
            part = jnp.dot(
                pick,
                normed[:, features(h * 2 + lo if near else tp)],
                preferred_element_type=F32,
            ).astype(BF16)
            for i, q in enumerate(targets):
                send[q, h] = part[i * cap : (i + 1) * cap]

    def launch(targets):
        for q in targets:
            a2a(q).start()

    def core_copy(q):
        block = rows.at[peer(q), lo]
        return pltpu.make_async_remote_copy(
            src_ref=block,
            dst_ref=block,
            send_sem=core_s.at[q],
            recv_sem=core_r.at[q],
            device_id=(me, partner),
            device_id_type=MESH,
        )

    def core_in(q):
        block = rows.at[peer(q), 1 - lo]
        return pltpu.make_async_remote_copy(
            src_ref=block,
            dst_ref=block,
            send_sem=core_s.at[q],
            recv_sem=core_r.at[q],
            device_id=(me, partner),
            device_id_type=MESH,
        )

    def x_copy(q, outgoing=True):
        block = rows.at[peer(q), lo, hi if outgoing else 1 - hi]
        return pltpu.make_async_remote_copy(
            src_ref=block,
            dst_ref=block,
            send_sem=x_s.at[q],
            recv_sem=x_r.at[q],
            device_id=(me, opposite),
            device_id_type=MESH,
        )

    def hid_copy(g, d, outgoing=True):
        t = sibling(d)
        span = pl.ds(0, len(groups[g]) * cap)
        return pltpu.make_async_remote_copy(
            src_ref=hid.at[g, tp, span],
            dst_ref=hid.at[g, tp if outgoing else t, span],
            send_sem=hid_s.at[g, d],
            recv_sem=hid_r.at[g, d],
            device_id=(me, t),
            device_id_type=MESH,
        )

    def ret_copy(q, outgoing=True):
        p = peer(q)
        owner = me if outgoing else p
        return pltpu.make_async_remote_copy(
            src_ref=back_out.at[q],
            dst_ref=back_in.at[owner],
            send_sem=ret_s.at[q],
            recv_sem=ret_r.at[owner],
            device_id=(p, tp),
            device_id_type=MESH,
        )

    def sh_core_copy():
        return pltpu.make_async_remote_copy(
            src_ref=sh_terms.at[1 - lo],
            dst_ref=sh_core_in,
            send_sem=sh_s.at[0],
            recv_sem=sh_r.at[0],
            device_id=(me, partner),
            device_id_type=MESH,
        )

    def sh_x_copy():
        return pltpu.make_async_remote_copy(
            src_ref=sh_x_out,
            dst_ref=sh_x_in,
            send_sem=sh_s.at[1],
            recv_sem=sh_r.at[1],
            device_id=(me, opposite),
            device_id_type=MESH,
        )

    def hidden_of(mixed):
        gate, up = mixed[:, :ff], mixed[:, ff:]
        return (gate / (1.0 + jnp.exp(-gate)) * up).astype(BF16)

    def make_picks():
        lines = [rank_t[pl.ds(peer(q), 1), :] for q in range(n)]
        for q in range(n):
            p = peer(q)
            weight = jnp.zeros((1, tok), F32)
            for k in range(chosen):
                weight = weight + jnp.where(ids[k] == p, weights[k], 0.0)
            lines.append(weight)
        at_row = lax.broadcasted_iota(jnp.int32, (tok, tok), 0)
        table = jnp.zeros((tok, tok), F32)
        for index, line in enumerate(lines):
            table = jnp.where(at_row == index, line, table)
        table = table.T
        cols[...] = table
        slot = lax.broadcasted_iota(jnp.int32, (tok, cap), 1).astype(F32)
        for q in range(n):
            picks[q] = jnp.where(slot == table[:, q : q + 1], 1.0, 0.0).astype(BF16)

    for g in (FAR_A, FAR_B):
        fill(away(g))
    pl.semaphore_wait(barrier, n - 1 + n_tp - 1)
    for g in (FAR_A, FAR_B):
        launch(away(g))
    for d in (2, 3):
        weight_copy(d).start()
    for g in (NEAR_Z, NEAR_Y):
        if away(g):
            fill(away(g))
            launch(away(g))
    weight_copy(1).start()

    for load in loads[:3]:
        load.wait()
    sh_hidden = hidden_of(jnp.dot(normed[...], sw_in[...], preferred_element_type=F32))
    for t in range(n_tp):
        sh_terms[t % 2, t // 2] = jnp.dot(
            sh_hidden, sw_out[:, pl.ds(t * share, share)], preferred_element_type=F32
        ).astype(BF16)
    sh_core_copy().start()
    own = pick_rows(0)
    for t in range(n_tp):
        rows[me, t % 2, t // 2] = jnp.dot(
            own, normed[:, pl.ds(t * share, share)], preferred_element_type=F32
        ).astype(BF16)
    make_picks()
    for load in loads[3:5]:
        load.wait()

    def shared(stage):
        if stage == 1:
            sh_core_copy().wait_recv()
            sh_x_out[...] = (
                sh_terms[lo, 1 - hi].astype(F32) + sh_core_in[1 - hi].astype(F32)
            ).astype(BF16)
            sh_x_copy().start()
            acc[...] = sh_terms[lo, hi].astype(F32) + sh_core_in[hi].astype(F32)
        else:
            sh_x_copy().wait_recv()
            acc[...] += sh_x_in[...].astype(F32)

    def arrive(g):
        for q in away(g):
            a2a(q, False).wait_recv()
            if q < half:
                core_copy(q).start()
            else:
                x_copy(q).start()

    def crossed(g):
        for q in away(g):
            x_copy(q, False).wait_recv()
            core_copy(q).start()

    def hidden(g):
        for q in away(g):
            core_in(q).wait_recv()
        total = jnp.zeros((len(groups[g]) * cap, 2 * ff), F32)
        for t in range(n_tp):
            block = jnp.concatenate(
                [rows[peer(q), t % 2, t // 2] for q in groups[g]], axis=0
            )
            total = total + jnp.dot(
                block, w_in[pl.ds(t * share, share), :], preferred_element_type=F32
            )
        hid[g, tp, pl.ds(0, len(groups[g]) * cap), :] = hidden_of(total)
        for d in (2, 3, 1):
            hid_copy(g, d).start()

    placed = []

    def down(g):
        if not placed:
            loads[5].wait()
            for d in range(1, n_tp):
                weight_copy(d, False).wait_recv()
            placed.append(True)
        for d in range(1, n_tp):
            hid_copy(g, d, False).wait_recv()
        block = jnp.concatenate(
            [hid[g, t, pl.ds(0, len(groups[g]) * cap), :] for t in range(n_tp)], axis=1
        )
        total = jnp.dot(
            block, w_dn[...].reshape(n_tp * ff, share), preferred_element_type=F32
        ).astype(BF16)
        for i, q in enumerate(groups[g]):
            part = total[i * cap : (i + 1) * cap]
            if q == 0:
                back_in[me] = part
            else:
                back_out[q] = part
                ret_copy(q).start()

    def add(g):
        total = acc[...]
        for q in groups[g]:
            if q > 0:
                ret_copy(q, False).wait_recv()
            total = total + cols[:, n + q : n + q + 1] * jnp.dot(
                picks[q], back_in[peer(q)], preferred_element_type=F32
            )
        if g == ORDER[-1][1]:
            out_ref[...] = total.astype(BF16)
        else:
            acc[...] = total

    steps = dict(
        shared=shared, arrive=arrive, crossed=crossed, hidden=hidden, down=down, add=add
    )
    for name, which in ORDER:
        steps[name](which)

    for q in range(1, n):
        a2a(q).wait_send()
        core_copy(q).wait_send()
        ret_copy(q).wait_send()
        if q >= half:
            x_copy(q).wait_send()
    for g in range(len(groups)):
        for d in range(1, n_tp):
            hid_copy(g, d).wait_send()
    for d in range(1, n_tp):
        weight_copy(d).wait_send()
    sh_core_copy().wait_send()
    sh_x_copy().wait_send()


def local(
    tokens,
    norm_gain,
    expert_ids,
    route_weights,
    gate_weight,
    up_weight,
    down_weight,
    shared_gate,
    shared_up,
    shared_down,
):
    tok, width = tokens.shape
    chosen = expert_ids.shape[1]
    n = lax.axis_size("ep")
    n_tp = lax.axis_size("tp")
    local_experts, _, ff = gate_weight.shape
    fits = n & (n - 1) == 0 and 4 <= n <= 8 and n_tp == 4 and local_experts == 1
    if not fits:
        return wide_local(
            tokens,
            norm_gain,
            expert_ids,
            route_weights,
            gate_weight,
            up_weight,
            down_weight,
            shared_gate,
            shared_up,
            shared_down,
        )
    cap = round_up((3 * tok * chosen + 2 * n - 1) // (2 * n), 16)
    share = width // n_tp
    pair = n // 4
    blocks = len(split(n))
    hbm = pl.BlockSpec(memory_space=pltpu.HBM)
    dma = pltpu.SemaphoreType.DMA
    return pl.pallas_call(
        functools.partial(paired_kernel, n, n_tp, cap),
        out_shape=pltpu.VMEM((tok, share), BF16),
        in_specs=[hbm] * 10,
        out_specs=pl.BlockSpec(memory_space=pltpu.VMEM),
        scratch_shapes=[
            pltpu.VMEM((tok, width), BF16),
            pltpu.VMEM((width,), BF16),
            pltpu.VMEM((chosen, tok), jnp.int32),
            pltpu.VMEM((chosen, tok), F32),
            pltpu.VMEM((width, 2 * ff), BF16),
            pltpu.VMEM((n_tp, ff, share), BF16),
            pltpu.VMEM((width, 2 * ff), BF16),
            pltpu.VMEM((ff, width), BF16),
            pltpu.VMEM((tok, width), BF16),
            pltpu.VMEM((round_up(n, 128), tok), F32),
            pltpu.VMEM((tok, tok), F32),
            pltpu.VMEM((n, tok, cap), BF16),
            pltpu.VMEM((n, 2, cap, share), BF16),
            pltpu.VMEM((n, 2, 2, cap, share), BF16),
            pltpu.VMEM((blocks, n_tp, pair * cap, ff), BF16),
            pltpu.VMEM((n, cap, share), BF16),
            pltpu.VMEM((n, cap, share), BF16),
            pltpu.VMEM((tok, share), F32),
            pltpu.VMEM((2, 2, tok, share), BF16),
            pltpu.VMEM((2, tok, share), BF16),
            pltpu.VMEM((tok, share), BF16),
            pltpu.VMEM((tok, share), BF16),
            dma((4,)),
            dma((6,)),
            dma((n,)),
            dma((n,)),
            dma((n,)),
            dma((n,)),
            dma((n,)),
            dma((n,)),
            dma((n_tp,)),
            dma((n_tp,)),
            dma((blocks, n_tp)),
            dma((blocks, n_tp)),
            dma((n,)),
            dma((n,)),
            dma((2,)),
            dma((2,)),
        ],
        compiler_params=pltpu.CompilerParams(
            collective_id=0, has_side_effects=True, vmem_limit_bytes=60000000
        ),
        name="moe",
    )(
        tokens,
        norm_gain,
        expert_ids.T,
        route_weights.T,
        gate_weight,
        up_weight,
        down_weight,
        shared_gate,
        shared_up,
        shared_down,
    )


def solution(mesh):
    in_specs = (
        P("ep", None),
        P(),
        P("ep", None),
        P("ep", None),
        P("ep", None, "tp"),
        P("ep", None, "tp"),
        P("ep", "tp", None),
        P(None, "tp"),
        P(None, "tp"),
        P("tp", None),
    )
    out_specs = P("ep", "tp")
    return jax.shard_map(local, mesh=mesh, in_specs=in_specs, out_specs=out_specs, check_vma=False)
```

```python
import functools

import jax
import jax.numpy as jnp
from jax import lax
from jax.experimental import pallas as pl
from jax.experimental.pallas import tpu as pltpu
from jax.sharding import PartitionSpec as P

norm_eps = 1e-06
MESH = pl.DeviceIdType.MESH
ARRIVE, SPACING, SHARED = 2.7, 1.3, 2.0
LATENCY = (0.0, 4.0, 1.5, 2.5, 4.0)
F32, BF16 = jnp.float32, jnp.bfloat16


def round_up(value, unit):
    return (value + unit - 1) // unit * unit


def wide_kernel(
    n,
    n_tp,
    experts,
    cap,
    tokens_ref,
    gain_ref,
    ids_ref,
    rw_ref,
    wg_ref,
    wu_ref,
    wd_ref,
    sg_ref,
    su_ref,
    sd_ref,
    out_ref,
    tokens,
    gain,
    ids_v,
    rw_v,
    out_v,
    w_in,
    w_out,
    sw_in,
    sw_out,
    normed,
    rank_t,
    picks,
    send,
    rows,
    terms,
    core_in,
    x_out,
    x_in,
    back_out,
    back_in,
    sh_terms,
    sh_core_in,
    sh_x_out,
    sh_x_in,
    in_sem,
    w_sem,
    a2a_s,
    a2a_r,
    core_s,
    core_r,
    x_s,
    x_r,
    fwd_s,
    fwd_r,
    rsc_s,
    rsc_r,
    rsx_s,
    rsx_r,
    ret_s,
    ret_r,
    sh_s,
    sh_r,
):
    tok, width = tokens_ref.shape
    share = width // n_tp
    local_experts, _, ff = wg_ref.shape
    chosen = ids_ref.shape[0]
    halves = n_tp // 2
    me = lax.axis_index("ep")
    tp = lax.axis_index("tp")
    hi, lo = tp // 2, tp % 2
    partner = hi * 2 + 1 - lo

    def across(d):
        return (hi + d) % halves

    def steps(body):
        if n <= 8:
            for j in range(n):
                body(j)
        else:

            def one(j, carry):
                body(j)
                return carry

            lax.fori_loop(0, n, one, 0)

    def mirror(j):
        total, bit = 0, 1
        while bit < n:
            total = total + ((me // bit + j // bit) % 2) * bit
            bit *= 2
        return total

    even = n & (n - 1) == 0

    def source(j):
        return mirror(j) if even else (me - j + n) % n

    def target(j):
        return mirror(j) if even else (me + j) % n

    def when(cond, body):
        if isinstance(cond, bool):
            if cond:
                body()
        else:
            pl.when(cond)(body)

    firsts = [
        pltpu.make_async_copy(tokens_ref, tokens, in_sem.at[0]),
        pltpu.make_async_copy(gain_ref, gain, in_sem.at[1]),
        pltpu.make_async_copy(ids_ref, ids_v, in_sem.at[2]),
        pltpu.make_async_copy(rw_ref, rw_v, in_sem.at[3]),
    ]
    for load in firsts:
        load.start()

    barrier = pltpu.get_barrier_semaphore()

    def greet(j):
        def go():
            pl.semaphore_signal(barrier, inc=1, device_id=(target(j), tp), device_id_type=MESH)

        when(j > 0, go)

    steps(greet)
    pl.semaphore_signal(barrier, inc=1, device_id=(me, partner), device_id_type=MESH)
    for d in range(1, halves):
        pl.semaphore_signal(
            barrier, inc=1, device_id=(me, across(d) * 2 + lo), device_id_type=MESH
        )

    loads = [
        pltpu.make_async_copy(sg_ref, sw_in.at[:, pl.ds(0, ff)], w_sem.at[0]),
        pltpu.make_async_copy(su_ref, sw_in.at[:, pl.ds(ff, ff)], w_sem.at[1]),
        pltpu.make_async_copy(sd_ref, sw_out, w_sem.at[2]),
        pltpu.make_async_copy(wg_ref, w_in.at[:, :, pl.ds(0, ff)], w_sem.at[3]),
        pltpu.make_async_copy(wu_ref, w_in.at[:, :, pl.ds(ff, ff)], w_sem.at[4]),
        pltpu.make_async_copy(wd_ref, w_out, w_sem.at[5]),
    ]
    for load in loads:
        load.start()

    firsts[2].wait()
    firsts[3].wait()
    lanes = rank_t.shape[0]
    ids = [ids_v[k : k + 1, :] for k in range(chosen)]
    weights = [rw_v[k : k + 1, :] for k in range(chosen)]
    expert = lax.broadcasted_iota(jnp.int32, (lanes, tok), 0)
    named = ids[0] == expert
    for k in range(1, chosen):
        named = named | (ids[k] == expert)
    earlier = lax.broadcasted_iota(jnp.int32, (tok, tok), 0) < lax.broadcasted_iota(
        jnp.int32, (tok, tok), 1
    )
    rank = jnp.dot(
        jnp.where(named, 1.0, 0.0).astype(BF16),
        jnp.where(earlier, 1.0, 0.0).astype(BF16),
        preferred_element_type=F32,
    )
    rank_t[...] = jnp.where(named, rank, -1.0)

    firsts[0].wait()
    firsts[1].wait()
    values = tokens[...].astype(F32)
    scale = lax.rsqrt(jnp.mean(values * values, axis=-1, keepdims=True) + norm_eps)
    normed[...] = (values * scale * gain[...].astype(F32).reshape(1, width)).astype(BF16)

    chunk = local_experts * cap
    slot_row = lax.broadcasted_iota(jnp.int32, (cap, tok), 0).astype(F32)
    column = pl.ds(pl.multiple_of(tp * share, 128), share)

    def dispatch(j, features):
        p = target(j)
        parts = []
        for le in range(local_experts):
            line = rank_t[pl.ds(p * local_experts + le, 1), :]
            pick = jnp.where(slot_row == line, 1.0, 0.0).astype(BF16)
            parts.append(
                jnp.dot(pick, normed[:, features], preferred_element_type=F32).astype(BF16)
            )
        return parts

    def a2a(j):
        return pltpu.make_async_remote_copy(
            src_ref=send.at[j],
            dst_ref=rows.at[me, tp],
            send_sem=a2a_s.at[j],
            recv_sem=a2a_r.at[me],
            device_id=(target(j), tp),
            device_id_type=MESH,
        )

    def a2a_in(j):
        s = source(j)
        return pltpu.make_async_remote_copy(
            src_ref=send.at[j],
            dst_ref=rows.at[s, tp],
            send_sem=a2a_s.at[j],
            recv_sem=a2a_r.at[s],
            device_id=(target(j), tp),
            device_id_type=MESH,
        )

    pl.semaphore_wait(barrier, (n - 1) + 1 + (halves - 1))

    def dispatch_and_send(j):
        def go():
            for le, part in enumerate(dispatch(j, column)):
                send[j, pl.ds(le * cap, cap), :] = part
            a2a(j).start()

        when(j > 0, go)

    steps(dispatch_and_send)

    def core_copy(j):
        s = source(j)
        return pltpu.make_async_remote_copy(
            src_ref=rows.at[s, tp],
            dst_ref=rows.at[s, tp],
            send_sem=core_s.at[j],
            recv_sem=core_r.at[j],
            device_id=(me, partner),
            device_id_type=MESH,
        )

    def x_copy(j, d):
        s = source(j)
        return pltpu.make_async_remote_copy(
            src_ref=rows.at[s, tp],
            dst_ref=rows.at[s, tp],
            send_sem=x_s.at[j, d - 1],
            recv_sem=x_r.at[j, d - 1],
            device_id=(me, across(d) * 2 + lo),
            device_id_type=MESH,
        )

    def fwd_copy(j, d):
        s = source(j)
        held = across(halves - d) * 2 + lo
        return pltpu.make_async_remote_copy(
            src_ref=rows.at[s, held],
            dst_ref=rows.at[s, held],
            send_sem=fwd_s.at[j, d - 1],
            recv_sem=fwd_r.at[j, d - 1],
            device_id=(me, partner),
            device_id_type=MESH,
        )

    def stage_a(j):
        a2a_in(j).wait_recv()
        for d in range(1, halves):
            x_copy(j, d).start()
        core_copy(j).start()

    def stage_b(j):
        for d in range(1, halves):
            x_copy(j, d).wait_recv()
            fwd_copy(j, d).start()

    def rsc_copy(j):
        return pltpu.make_async_remote_copy(
            src_ref=terms.at[j, 1 - lo],
            dst_ref=core_in.at[j],
            send_sem=rsc_s.at[j],
            recv_sem=rsc_r.at[j],
            device_id=(me, partner),
            device_id_type=MESH,
        )

    def rsx_copy(j, d):
        return pltpu.make_async_remote_copy(
            src_ref=x_out.at[j, d - 1],
            dst_ref=x_in.at[j, d - 1],
            send_sem=rsx_s.at[j, d - 1],
            recv_sem=rsx_r.at[j, d - 1],
            device_id=(me, across(d) * 2 + lo),
            device_id_type=MESH,
        )

    def ret_copy(j):
        return pltpu.make_async_remote_copy(
            src_ref=back_out.at[j],
            dst_ref=back_in.at[me],
            send_sem=ret_s.at[j],
            recv_sem=ret_r.at[me],
            device_id=(source(j), tp),
            device_id_type=MESH,
        )

    def ret_in(j):
        g = target(j)
        return pltpu.make_async_remote_copy(
            src_ref=back_out.at[j],
            dst_ref=back_in.at[g],
            send_sem=ret_s.at[j],
            recv_sem=ret_r.at[g],
            device_id=(source(j), tp),
            device_id_type=MESH,
        )

    def hidden_of(mixed):
        gate, up = mixed[:, :ff], mixed[:, ff:]
        return (gate / (1.0 + jnp.exp(-gate)) * up).astype(BF16)

    def expert_hidden(s, le):
        total = jnp.zeros((cap, 2 * ff), F32)
        for t in range(n_tp):
            total = total + jnp.dot(
                rows[s, t, pl.ds(le * cap, cap), :],
                w_in[le, pl.ds(t * share, share), :],
                preferred_element_type=F32,
            )
        return hidden_of(total)

    def stage_c(j):
        core_copy(j).wait_recv()
        for d in range(1, halves):
            fwd_copy(j, d).wait_recv()
        for le in range(local_experts):
            hidden = expert_hidden(source(j), le)
            for t in range(n_tp):
                terms[j, t % 2, t // 2, pl.ds(le * cap, cap), :] = jnp.dot(
                    hidden,
                    w_out[le, :, pl.ds(t * share, share)],
                    preferred_element_type=F32,
                ).astype(BF16)
        rsc_copy(j).start()

    def stage_d(j):
        rsc_copy(j).wait_recv()
        for d in range(1, halves):
            h = across(d)
            x_out[j, d - 1] = (
                terms[j, lo, h].astype(F32) + core_in[j, h].astype(F32)
            ).astype(BF16)
            rsx_copy(j, d).start()

    def stage_e(j):
        total = terms[j, lo, hi].astype(F32) + core_in[j, hi].astype(F32)
        for d in range(1, halves):
            rsx_copy(j, d).wait_recv()
            total = total + x_in[j, d - 1].astype(F32)
        back_out[j] = total.astype(BF16)

        ret_copy(j).start()

    def sh_core_copy():
        return pltpu.make_async_remote_copy(
            src_ref=sh_terms.at[1 - lo],
            dst_ref=sh_core_in,
            send_sem=sh_s.at[0],
            recv_sem=sh_r.at[0],
            device_id=(me, partner),
            device_id_type=MESH,
        )

    def sh_x_copy(d):
        return pltpu.make_async_remote_copy(
            src_ref=sh_x_out.at[d - 1],
            dst_ref=sh_x_in.at[d - 1],
            send_sem=sh_s.at[d],
            recv_sem=sh_r.at[d],
            device_id=(me, across(d) * 2 + lo),
            device_id_type=MESH,
        )

    def make_picks():
        slots = n * chunk
        place = rank + (expert * cap).astype(F32)
        lines = [
            jnp.sum(jnp.where(ids[k] == expert, place, 0.0), axis=0, keepdims=True)
            for k in range(chosen)
        ] + weights
        for le in range(local_experts):
            mine = me * local_experts + le
            lines.append(rank_t[pl.ds(mine, 1), :])
            weight = jnp.zeros((1, tok), F32)
            for k in range(chosen):
                weight = weight + jnp.where(ids[k] == mine, weights[k], 0.0)
            lines.append(weight)
        at_row = lax.broadcasted_iota(jnp.int32, (tok, tok), 0)
        table = jnp.zeros((tok, tok), F32)
        for index, line in enumerate(lines):
            table = jnp.where(at_row == index, line, table)
        table = table.T
        spot = lax.broadcasted_iota(jnp.int32, (tok, slots), 1).astype(F32)
        for k in range(chosen):
            picks[k] = jnp.where(spot == table[:, k : k + 1], 1.0, 0.0).astype(BF16)
        return table

    def shared_first():
        for load in loads[:3]:
            load.wait()
        hidden = hidden_of(jnp.dot(normed[...], sw_in[...], preferred_element_type=F32))
        slot = lax.broadcasted_iota(jnp.int32, (tok, cap), 1).astype(F32)
        table = make_picks()
        for load in loads[3:]:
            load.wait()
        own = []
        for le in range(local_experts):
            for t in range(n_tp):
                features = pl.ds(t * share, share)
                rows[me, t, pl.ds(le * cap, cap), :] = dispatch(0, features)[le]
            own.append(expert_hidden(me, le))
        for t in range(n_tp):
            features = pl.ds(t * share, share)
            total = jnp.dot(hidden, sw_out[:, features], preferred_element_type=F32)
            for le in range(local_experts):
                at = 2 * chosen + 2 * le
                pick = jnp.where(slot == table[:, at : at + 1], 1.0, 0.0).astype(BF16)
                term = jnp.dot(
                    own[le], w_out[le, :, features], preferred_element_type=F32
                ).astype(BF16)
                total = total + table[:, at + 1 : at + 2] * jnp.dot(
                    pick, term, preferred_element_type=F32
                )
            sh_terms[t % 2, t // 2] = total.astype(BF16)
        sh_core_copy().start()
        return [table[:, chosen + k : chosen + k + 1] for k in range(chosen)]

    def shared_second():
        sh_core_copy().wait_recv()
        for d in range(1, halves):
            h = across(d)
            sh_x_out[d - 1] = (sh_terms[lo, h].astype(F32) + sh_core_in[h].astype(F32)).astype(
                BF16
            )
            sh_x_copy(d).start()

    back_in[me] = jnp.zeros((chunk, share), BF16)
    route = shared_first()

    stages = (stage_a, stage_b, stage_c, stage_d, stage_e)

    if n <= 8:
        order = []
        for j in range(1, n):
            at = ARRIVE + SPACING * (j - 1)
            for index, stage in enumerate(stages):
                at += LATENCY[index]
                order.append((at, index, j))
        order.append((SHARED, -1, 0))
        for _, index, j in sorted(order):
            if index < 0:
                shared_second()
            else:
                stages[index](j)
    else:
        shared_second()
        lags = (0, 2, 3, 4, 6)

        def one(i, carry):
            for lag, stage in zip(lags, stages):
                pl.when((i - lag >= 1) & (i - lag < n))(functools.partial(stage, i - lag))
            return carry

        lax.fori_loop(1, n + lags[-1], one, 0)

    total = sh_terms[lo, hi].astype(F32) + sh_core_in[hi].astype(F32)
    for d in range(1, halves):
        sh_x_copy(d).wait_recv()
        total = total + sh_x_in[d - 1].astype(F32)

    steps(lambda j: when(j > 0, lambda: ret_in(j).wait_recv()))
    came = back_in[...].reshape(n * chunk, share)
    for k in range(chosen):
        total = total + route[k] * jnp.dot(
            picks[k], came, preferred_element_type=F32
        )
    out_v[...] = total.astype(BF16)
    result = pltpu.make_async_copy(out_v, out_ref, in_sem.at[0])
    result.start()

    def drain(j):
        def far():
            a2a(j).wait_send()
            ret_copy(j).wait_send()

            core_copy(j).wait_send()
            rsc_copy(j).wait_send()
            for d in range(1, halves):
                x_copy(j, d).wait_send()
                fwd_copy(j, d).wait_send()
                rsx_copy(j, d).wait_send()

        when(j > 0, far)

    steps(drain)
    sh_core_copy().wait_send()
    for d in range(1, halves):
        sh_x_copy(d).wait_send()
    result.wait()


def wide_local(
    tokens,
    norm_gain,
    expert_ids,
    route_weights,
    gate_weight,
    up_weight,
    down_weight,
    shared_gate,
    shared_up,
    shared_down,
):
    tok, width = tokens.shape
    chosen = expert_ids.shape[1]
    n = lax.axis_size("ep")
    n_tp = lax.axis_size("tp")
    local_experts, _, ff = gate_weight.shape
    experts = n * local_experts
    cap = round_up((3 * tok * chosen + 2 * experts - 1) // (2 * experts), 16)
    share = width // n_tp
    halves = n_tp // 2
    chunk = local_experts * cap
    others = max(halves - 1, 1)
    hbm = pl.BlockSpec(memory_space=pltpu.HBM)
    dma = pltpu.SemaphoreType.DMA
    body = functools.partial(wide_kernel, n, n_tp, experts, cap)
    return pl.pallas_call(
        body,
        out_shape=jax.ShapeDtypeStruct((tok, share), BF16),
        in_specs=[hbm] * 10,
        out_specs=pl.BlockSpec(memory_space=pl.ANY),
        scratch_shapes=[
            pltpu.VMEM((tok, width), BF16),
            pltpu.VMEM((width,), BF16),
            pltpu.VMEM((chosen, tok), jnp.int32),
            pltpu.VMEM((chosen, tok), F32),
            pltpu.VMEM((tok, share), BF16),
            pltpu.VMEM((local_experts, width, 2 * ff), BF16),
            pltpu.VMEM((local_experts, ff, width), BF16),
            pltpu.VMEM((width, 2 * ff), BF16),
            pltpu.VMEM((ff, width), BF16),
            pltpu.VMEM((tok, width), BF16),
            pltpu.VMEM((round_up(experts, 128), tok), F32),
            pltpu.VMEM((chosen, tok, n * chunk), BF16),
            pltpu.VMEM((n, chunk, share), BF16),
            pltpu.VMEM((n, n_tp, chunk, share), BF16),
            pltpu.VMEM((n, 2, halves, chunk, share), BF16),
            pltpu.VMEM((n, halves, chunk, share), BF16),
            pltpu.VMEM((n, others, chunk, share), BF16),
            pltpu.VMEM((n, others, chunk, share), BF16),
            pltpu.VMEM((n, chunk, share), BF16),
            pltpu.VMEM((n, chunk, share), BF16),
            pltpu.VMEM((2, halves, tok, share), BF16),
            pltpu.VMEM((halves, tok, share), BF16),
            pltpu.VMEM((others, tok, share), BF16),
            pltpu.VMEM((others, tok, share), BF16),
            dma((4,)),
            dma((6,)),
            dma((n,)),
            dma((n,)),
            dma((n,)),
            dma((n,)),
            dma((n, others)),
            dma((n, others)),
            dma((n, others)),
            dma((n, others)),
            dma((n,)),
            dma((n,)),
            dma((n, others)),
            dma((n, others)),
            dma((n,)),
            dma((n,)),
            dma((halves,)),
            dma((halves,)),
        ],
        compiler_params=pltpu.CompilerParams(
            collective_id=0, has_side_effects=True, vmem_limit_bytes=67043328 - 3 * tok * share
        ),
        name="moe",
    )(
        tokens,
        norm_gain,
        expert_ids.T,
        route_weights.T,
        gate_weight,
        up_weight,
        down_weight,
        shared_gate,
        shared_up,
        shared_down,
    )


NEAR_Z, NEAR_Y, FAR_A, FAR_B = range(4)
ORDER = (
    ("shared", 1),
    ("arrive", FAR_A),
    ("arrive", NEAR_Z),
    ("arrive", FAR_B),
    ("arrive", NEAR_Y),
    ("crossed", FAR_A),
    ("hidden", NEAR_Z),
    ("hidden", FAR_A),
    ("hidden", NEAR_Y),
    ("crossed", FAR_B),
    ("hidden", FAR_B),
    ("down", NEAR_Z),
    ("down", FAR_A),
    ("down", NEAR_Y),
    ("down", FAR_B),
    ("shared", 2),
    ("add", NEAR_Z),
    ("add", NEAR_Y),
    ("add", FAR_A),
    ("add", FAR_B),
)


def split(n):
    half, pair = n // 2, n // 4
    return [
        tuple(range(pair, half)),
        tuple(range(pair)),
        tuple(range(half, half + pair)),
        tuple(range(half + pair, n)),
    ]


def paired_kernel(
    n,
    n_tp,
    cap,
    tokens_ref,
    gain_ref,
    ids_ref,
    rw_ref,
    wg_ref,
    wu_ref,
    wd_ref,
    sg_ref,
    su_ref,
    sd_ref,
    out_ref,
    tokens,
    gain,
    ids_v,
    rw_v,
    w_in,
    w_dn,
    sw_in,
    sw_out,
    normed,
    rank_t,
    cols,
    picks,
    send,
    rows,
    hid,
    back_out,
    back_in,
    acc,
    sh_terms,
    sh_core_in,
    sh_x_out,
    sh_x_in,
    in_sem,
    w_sem,
    a2a_s,
    a2a_r,
    core_s,
    core_r,
    x_s,
    x_r,
    wd_s,
    wd_r,
    hid_s,
    hid_r,
    ret_s,
    ret_r,
    sh_s,
    sh_r,
):
    tok, width = tokens_ref.shape
    share = width // n_tp
    ff = wg_ref.shape[2]
    chosen = ids_ref.shape[0]
    half, pair = n // 2, n // 4
    groups = split(n)
    me = lax.axis_index("ep")
    tp = lax.axis_index("tp")
    hi, lo = tp // 2, tp % 2
    partner = hi * 2 + 1 - lo
    opposite = (1 - hi) * 2 + lo

    def peer(q):
        total, bit = 0, 1
        while bit < n:
            total = total + ((me // bit + q // bit) % 2) * bit
            bit *= 2
        return total

    def away(g):
        return [q for q in groups[g] if q > 0]

    def sibling(d):
        return (hi + d // 2) % 2 * 2 + (lo + d % 2) % 2

    firsts = [
        pltpu.make_async_copy(tokens_ref, tokens, in_sem.at[0]),
        pltpu.make_async_copy(gain_ref, gain, in_sem.at[1]),
        pltpu.make_async_copy(ids_ref, ids_v, in_sem.at[2]),
        pltpu.make_async_copy(rw_ref, rw_v, in_sem.at[3]),
    ]
    for load in firsts:
        load.start()

    barrier = pltpu.get_barrier_semaphore()
    for q in range(n - 1, 0, -1):
        pl.semaphore_signal(barrier, inc=1, device_id=(peer(q), tp), device_id_type=MESH)
    for d in range(1, n_tp):
        pl.semaphore_signal(barrier, inc=1, device_id=(me, sibling(d)), device_id_type=MESH)

    def features(t):
        return pl.ds(pl.multiple_of(t * share, 128), share)

    loads = [
        pltpu.make_async_copy(sg_ref, sw_in.at[:, pl.ds(0, ff)], w_sem.at[0]),
        pltpu.make_async_copy(su_ref, sw_in.at[:, pl.ds(ff, ff)], w_sem.at[1]),
        pltpu.make_async_copy(sd_ref, sw_out, w_sem.at[2]),
        pltpu.make_async_copy(wg_ref.at[0], w_in.at[:, pl.ds(0, ff)], w_sem.at[3]),
        pltpu.make_async_copy(wu_ref.at[0], w_in.at[:, pl.ds(ff, ff)], w_sem.at[4]),
        pltpu.make_async_copy(wd_ref.at[0, :, features(tp)], w_dn.at[tp], w_sem.at[5]),
    ]
    for load in loads:
        load.start()

    firsts[2].wait()
    firsts[3].wait()
    lanes = rank_t.shape[0]
    ids = [ids_v[k : k + 1, :] for k in range(chosen)]
    weights = [rw_v[k : k + 1, :] for k in range(chosen)]
    expert = lax.broadcasted_iota(jnp.int32, (lanes, tok), 0)
    named = ids[0] == expert
    for k in range(1, chosen):
        named = named | (ids[k] == expert)
    earlier = lax.broadcasted_iota(jnp.int32, (tok, tok), 0) < lax.broadcasted_iota(
        jnp.int32, (tok, tok), 1
    )
    rank = jnp.dot(
        jnp.where(named, 1.0, 0.0).astype(BF16),
        jnp.where(earlier, 1.0, 0.0).astype(BF16),
        preferred_element_type=F32,
    )
    rank_t[...] = jnp.where(named, rank, -1.0)

    firsts[0].wait()
    firsts[1].wait()
    values = tokens[...].astype(F32)
    scale = lax.rsqrt(jnp.mean(values * values, axis=-1, keepdims=True) + norm_eps)
    normed[...] = (values * scale * gain[...].astype(F32).reshape(1, width)).astype(BF16)

    slot_row = lax.broadcasted_iota(jnp.int32, (cap, tok), 0).astype(F32)

    def pick_rows(q):
        line = rank_t[pl.ds(peer(q), 1), :]
        return jnp.where(slot_row == line, 1.0, 0.0).astype(BF16)

    def a2a(q, outgoing=True):
        p = peer(q)
        owner = me if outgoing else p
        if q < half:
            src, dst = send.at[q], rows.at[owner, lo]
        else:
            src, dst = send.at[q, 0], rows.at[owner, lo, hi]
        return pltpu.make_async_remote_copy(
            src_ref=src,
            dst_ref=dst,
            send_sem=a2a_s.at[q],
            recv_sem=a2a_r.at[owner],
            device_id=(p, tp),
            device_id_type=MESH,
        )

    def weight_copy(d, outgoing=True):
        t = sibling(d)
        return pltpu.make_async_remote_copy(
            src_ref=wd_ref.at[0, :, features(t)],
            dst_ref=w_dn.at[tp if outgoing else t],
            send_sem=wd_s.at[d],
            recv_sem=wd_r.at[d],
            device_id=(me, t),
            device_id_type=MESH,
        )

    def fill(targets):
        near = targets[0] < half
        pick = jnp.concatenate([pick_rows(q) for q in targets], axis=0)
        for h in range(2) if near else (0,):
            part = jnp.dot(
                pick,
                normed[:, features(h * 2 + lo if near else tp)],
                preferred_element_type=F32,
            ).astype(BF16)
            for i, q in enumerate(targets):
                send[q, h] = part[i * cap : (i + 1) * cap]

    def launch(targets):
        for q in targets:
            a2a(q).start()

    def core_copy(q):
        block = rows.at[peer(q), lo]
        return pltpu.make_async_remote_copy(
            src_ref=block,
            dst_ref=block,
            send_sem=core_s.at[q],
            recv_sem=core_r.at[q],
            device_id=(me, partner),
            device_id_type=MESH,
        )

    def core_in(q):
        block = rows.at[peer(q), 1 - lo]
        return pltpu.make_async_remote_copy(
            src_ref=block,
            dst_ref=block,
            send_sem=core_s.at[q],
            recv_sem=core_r.at[q],
            device_id=(me, partner),
            device_id_type=MESH,
        )

    def x_copy(q, outgoing=True):
        block = rows.at[peer(q), lo, hi if outgoing else 1 - hi]
        return pltpu.make_async_remote_copy(
            src_ref=block,
            dst_ref=block,
            send_sem=x_s.at[q],
            recv_sem=x_r.at[q],
            device_id=(me, opposite),
            device_id_type=MESH,
        )

    def hid_copy(g, d, outgoing=True):
        t = sibling(d)
        span = pl.ds(0, len(groups[g]) * cap)
        return pltpu.make_async_remote_copy(
            src_ref=hid.at[g, tp, span],
            dst_ref=hid.at[g, tp if outgoing else t, span],
            send_sem=hid_s.at[g, d],
            recv_sem=hid_r.at[g, d],
            device_id=(me, t),
            device_id_type=MESH,
        )

    def ret_copy(q, outgoing=True):
        p = peer(q)
        owner = me if outgoing else p
        return pltpu.make_async_remote_copy(
            src_ref=back_out.at[q],
            dst_ref=back_in.at[owner],
            send_sem=ret_s.at[q],
            recv_sem=ret_r.at[owner],
            device_id=(p, tp),
            device_id_type=MESH,
        )

    def sh_core_copy():
        return pltpu.make_async_remote_copy(
            src_ref=sh_terms.at[1 - lo],
            dst_ref=sh_core_in,
            send_sem=sh_s.at[0],
            recv_sem=sh_r.at[0],
            device_id=(me, partner),
            device_id_type=MESH,
        )

    def sh_x_copy():
        return pltpu.make_async_remote_copy(
            src_ref=sh_x_out,
            dst_ref=sh_x_in,
            send_sem=sh_s.at[1],
            recv_sem=sh_r.at[1],
            device_id=(me, opposite),
            device_id_type=MESH,
        )

    def hidden_of(mixed):
        gate, up = mixed[:, :ff], mixed[:, ff:]
        return (gate / (1.0 + jnp.exp(-gate)) * up).astype(BF16)

    def make_picks():
        lines = [rank_t[pl.ds(peer(q), 1), :] for q in range(n)]
        for q in range(n):
            p = peer(q)
            weight = jnp.zeros((1, tok), F32)
            for k in range(chosen):
                weight = weight + jnp.where(ids[k] == p, weights[k], 0.0)
            lines.append(weight)
        at_row = lax.broadcasted_iota(jnp.int32, (tok, tok), 0)
        table = jnp.zeros((tok, tok), F32)
        for index, line in enumerate(lines):
            table = jnp.where(at_row == index, line, table)
        table = table.T
        cols[...] = table
        slot = lax.broadcasted_iota(jnp.int32, (tok, cap), 1).astype(F32)
        for q in range(n):
            picks[q] = jnp.where(slot == table[:, q : q + 1], 1.0, 0.0).astype(BF16)

    for g in (FAR_A, FAR_B):
        fill(away(g))
    pl.semaphore_wait(barrier, n - 1 + n_tp - 1)
    for g in (FAR_A, FAR_B):
        launch(away(g))
    for d in (2, 3):
        weight_copy(d).start()
    for g in (NEAR_Z, NEAR_Y):
        if away(g):
            fill(away(g))
            launch(away(g))
    weight_copy(1).start()

    for load in loads[:3]:
        load.wait()
    sh_hidden = hidden_of(jnp.dot(normed[...], sw_in[...], preferred_element_type=F32))
    for t in range(n_tp):
        sh_terms[t % 2, t // 2] = jnp.dot(
            sh_hidden, sw_out[:, pl.ds(t * share, share)], preferred_element_type=F32
        ).astype(BF16)
    sh_core_copy().start()
    own = pick_rows(0)
    for t in range(n_tp):
        rows[me, t % 2, t // 2] = jnp.dot(
            own, normed[:, pl.ds(t * share, share)], preferred_element_type=F32
        ).astype(BF16)
    make_picks()
    for load in loads[3:5]:
        load.wait()

    def shared(stage):
        if stage == 1:
            sh_core_copy().wait_recv()
            sh_x_out[...] = (
                sh_terms[lo, 1 - hi].astype(F32) + sh_core_in[1 - hi].astype(F32)
            ).astype(BF16)
            sh_x_copy().start()
            acc[...] = sh_terms[lo, hi].astype(F32) + sh_core_in[hi].astype(F32)
        else:
            sh_x_copy().wait_recv()
            acc[...] += sh_x_in[...].astype(F32)

    def arrive(g):
        for q in away(g):
            a2a(q, False).wait_recv()
            if q < half:
                core_copy(q).start()
            else:
                x_copy(q).start()

    def crossed(g):
        for q in away(g):
            x_copy(q, False).wait_recv()
            core_copy(q).start()

    def hidden(g):
        for q in away(g):
            core_in(q).wait_recv()
        total = jnp.zeros((len(groups[g]) * cap, 2 * ff), F32)
        for t in range(n_tp):
            block = jnp.concatenate(
                [rows[peer(q), t % 2, t // 2] for q in groups[g]], axis=0
            )
            total = total + jnp.dot(
                block, w_in[pl.ds(t * share, share), :], preferred_element_type=F32
            )
        hid[g, tp, pl.ds(0, len(groups[g]) * cap), :] = hidden_of(total)
        for d in (3, 2, 1):
            hid_copy(g, d).start()

    placed = []

    def down(g):
        if not placed:
            loads[5].wait()
            for d in range(1, n_tp):
                weight_copy(d, False).wait_recv()
            placed.append(True)
        for d in range(1, n_tp):
            hid_copy(g, d, False).wait_recv()
        block = jnp.concatenate(
            [hid[g, t, pl.ds(0, len(groups[g]) * cap), :] for t in range(n_tp)], axis=1
        )
        total = jnp.dot(
            block, w_dn[...].reshape(n_tp * ff, share), preferred_element_type=F32
        ).astype(BF16)
        for i, q in enumerate(groups[g]):
            part = total[i * cap : (i + 1) * cap]
            if q == 0:
                back_in[me] = part
            else:
                back_out[q] = part
                ret_copy(q).start()

    def add(g):
        total = acc[...]
        for q in groups[g]:
            if q > 0:
                ret_copy(q, False).wait_recv()
            total = total + cols[:, n + q : n + q + 1] * jnp.dot(
                picks[q], back_in[peer(q)], preferred_element_type=F32
            )
        if g == ORDER[-1][1]:
            out_ref[...] = total.astype(BF16)
        else:
            acc[...] = total

    steps = dict(
        shared=shared, arrive=arrive, crossed=crossed, hidden=hidden, down=down, add=add
    )
    for name, which in ORDER:
        steps[name](which)

    for q in range(1, n):
        a2a(q).wait_send()
        core_copy(q).wait_send()
        ret_copy(q).wait_send()
        if q >= half:
            x_copy(q).wait_send()
    for g in range(len(groups)):
        for d in range(1, n_tp):
            hid_copy(g, d).wait_send()
    for d in range(1, n_tp):
        weight_copy(d).wait_send()
    sh_core_copy().wait_send()
    sh_x_copy().wait_send()


def local(
    tokens,
    norm_gain,
    expert_ids,
    route_weights,
    gate_weight,
    up_weight,
    down_weight,
    shared_gate,
    shared_up,
    shared_down,
):
    tok, width = tokens.shape
    chosen = expert_ids.shape[1]
    n = lax.axis_size("ep")
    n_tp = lax.axis_size("tp")
    local_experts, _, ff = gate_weight.shape
    fits = n & (n - 1) == 0 and 4 <= n <= 8 and n_tp == 4 and local_experts == 1
    if not fits:
        return wide_local(
            tokens,
            norm_gain,
            expert_ids,
            route_weights,
            gate_weight,
            up_weight,
            down_weight,
            shared_gate,
            shared_up,
            shared_down,
        )
    cap = round_up((3 * tok * chosen + 2 * n - 1) // (2 * n), 16)
    share = width // n_tp
    pair = n // 4
    blocks = len(split(n))
    hbm = pl.BlockSpec(memory_space=pltpu.HBM)
    dma = pltpu.SemaphoreType.DMA
    return pl.pallas_call(
        functools.partial(paired_kernel, n, n_tp, cap),
        out_shape=pltpu.VMEM((tok, share), BF16),
        in_specs=[hbm] * 10,
        out_specs=pl.BlockSpec(memory_space=pltpu.VMEM),
        scratch_shapes=[
            pltpu.VMEM((tok, width), BF16),
            pltpu.VMEM((width,), BF16),
            pltpu.VMEM((chosen, tok), jnp.int32),
            pltpu.VMEM((chosen, tok), F32),
            pltpu.VMEM((width, 2 * ff), BF16),
            pltpu.VMEM((n_tp, ff, share), BF16),
            pltpu.VMEM((width, 2 * ff), BF16),
            pltpu.VMEM((ff, width), BF16),
            pltpu.VMEM((tok, width), BF16),
            pltpu.VMEM((round_up(n, 128), tok), F32),
            pltpu.VMEM((tok, tok), F32),
            pltpu.VMEM((n, tok, cap), BF16),
            pltpu.VMEM((n, 2, cap, share), BF16),
            pltpu.VMEM((n, 2, 2, cap, share), BF16),
            pltpu.VMEM((blocks, n_tp, pair * cap, ff), BF16),
            pltpu.VMEM((n, cap, share), BF16),
            pltpu.VMEM((n, cap, share), BF16),
            pltpu.VMEM((tok, share), F32),
            pltpu.VMEM((2, 2, tok, share), BF16),
            pltpu.VMEM((2, tok, share), BF16),
            pltpu.VMEM((tok, share), BF16),
            pltpu.VMEM((tok, share), BF16),
            dma((4,)),
            dma((6,)),
            dma((n,)),
            dma((n,)),
            dma((n,)),
            dma((n,)),
            dma((n,)),
            dma((n,)),
            dma((n_tp,)),
            dma((n_tp,)),
            dma((blocks, n_tp)),
            dma((blocks, n_tp)),
            dma((n,)),
            dma((n,)),
            dma((2,)),
            dma((2,)),
        ],
        compiler_params=pltpu.CompilerParams(
            collective_id=0, has_side_effects=True, vmem_limit_bytes=60000000
        ),
        name="moe",
    )(
        tokens,
        norm_gain,
        expert_ids.T,
        route_weights.T,
        gate_weight,
        up_weight,
        down_weight,
        shared_gate,
        shared_up,
        shared_down,
    )


def solution(mesh):
    in_specs = (
        P("ep", None),
        P(),
        P("ep", None),
        P("ep", None),
        P("ep", None, "tp"),
        P("ep", None, "tp"),
        P("ep", "tp", None),
        P(None, "tp"),
        P(None, "tp"),
        P("tp", None),
    )
    out_specs = P("ep", "tp")
    return jax.shard_map(local, mesh=mesh, in_specs=in_specs, out_specs=out_specs, check_vma=False)
```
